512 devices in a mesh: grp: 2 (over y), tp: 16 (over z), dp: 16 (over x, core).
Axes of the slice: x: 8, y: 2, z: 16, core: 2. Of those that a mesh axis runs over, the one named last changes fastest.
The devices are a block of a 8x16x16 slice.
Arguments:
- stream: bfloat16 [1024, 4096], P(('grp', 'tp'), 'dp'), parts along dimension 0, may hold values from -6 to 6
- lengths: int32 [64], P(('grp', 'dp')), parts along dimension 0, may hold values from 1 to 16, as said below
- input_norm_gain: float32 [2, 4096], P(None, 'dp'), may hold values from 0.1 to 1.9
- query_projection: bfloat16 [2, 4096, 2048], P(None, 'dp', 'tp'), may hold values from -0.09375 to 0.09375
- key_projection: bfloat16 [2, 4096, 2048], P(None, 'dp', 'tp'), may hold values from -0.09375 to 0.09375
- forget_gate_weight: bfloat16 [2, 4096, 2048], P(None, 'dp', 'tp'), may hold values from -0.09375 to 0.09375
- value_projection: bfloat16 [2, 4096, 4096], P(None, 'dp', 'tp'), may hold values from -0.09375 to 0.09375
- output_gate_weight: bfloat16 [2, 4096, 4096], P(None, 'dp', 'tp'), may hold values from -0.09375 to 0.09375
- forget_gate_bias: float32 [2, 2048], P(None, 'tp'), may hold values from -3 to 3
- extra_frame_decay: float32 [2, 1024, 2048], P(None, ('grp', 'dp'), 'tp'), parts along dimension 1, may hold values from -0.7 to 0, as said below
- head_norm_gain: float32 [2, 512], replicated, may hold values from 0.1 to 1.9
- output_projection: bfloat16 [2, 4096, 4096], P(None, 'tp', 'dp'), may hold values from -0.09375 to 0.09375
- memory: float32 [2, 64, 2048, 512], P(None, ('grp', 'dp'), 'tp'), parts along dimension 1, may hold values from -6 to 6
Outputs:
- stream_out: bfloat16 [1024, 4096], P(('grp', 'tp'), 'dp'), parts along dimension 0
- memory_out: float32 [2, 64, 2048, 512], P(None, ('grp', 'dp'), 'tp'), parts along dimension 1
The draws below stay inside these ranges and needn't reach their ends.
There are 2 independent parts, one for each index of `grp`. The reference program is written for one: setup_inputs(seed, part) draws one part's arguments, and reference() takes and returns one part's arrays. A program takes and returns all parts, laid end to end along the dimension named above; an argument that names none is the same for every part. Nothing has to cross between parts.
Inputs may be any that keep to these rules, and one draw needn't show every extreme that they name: `lengths`: live frames of each sequence; at least one sequence has all 16. `extra_frame_decay`: zero at most frames; at the others, for every key channel, a value from -0.7 to -0.22.
All inputs are finite; a program needn't handle non-finite values.
Results may differ from the reference program's by a relative error of at most 0.03.
Values may be sent and summed in bfloat16 or wider, within the bound.
No kernel may reach another device: no remote copies, remote signals or barrier semaphores. Data moves between devices by JAX's collectives and lax.ppermute only.
A program may use at most 64 MiB of HBM per device.

```python
import jax
import jax.numpy as jnp
from jax import lax

D = 4096
HEADS = 8
KEY_DIM = 256
VALUE_DIM = 512
BLOCK_LEN = 16
BATCH = 32
TOKENS = 512
KEYS = 2048
VALUES = 4096
N_TP = 16
N_DP = 16


def draw_lengths(key, part):
    base_key, full_key, spot_key = jax.random.split(jax.random.fold_in(key, 23), 3)
    base = jax.random.randint(base_key, (BATCH,), 1, BLOCK_LEN // 2 + 4, dtype=jnp.int32)
    full_pick = jax.random.randint(full_key, (BATCH,), 0, 6, dtype=jnp.int32) == 0
    lengths = jnp.where(full_pick, BLOCK_LEN, base)
    spot = jax.random.randint(spot_key, (), 0, BATCH, dtype=jnp.int32)
    lengths = jnp.where(jnp.arange(BATCH, dtype=jnp.int32) == spot, BLOCK_LEN, lengths)
    return jnp.minimum(lengths, BLOCK_LEN).astype(jnp.int32)


def draw_extra_frame_decay(key, part):
    hit_key, amount_key = jax.random.split(jax.random.fold_in(key, 11))
    struck = jax.random.uniform(hit_key, (2, TOKENS, 1), jnp.float32) < 0.12
    amounts = jax.random.uniform(amount_key, (2, TOKENS, KEYS), jnp.float32, -0.7, -0.22)
    return jnp.where(struck, amounts, 0.0).astype(jnp.float32)


def block_levels(key, shape, cuts, low, high):
    def one(axis_at, parts):
        steps = jax.random.uniform(jax.random.fold_in(jax.random.fold_in(key, 6), axis_at), (parts,), jnp.float32, low / len(cuts), high / len(cuts))
        return jnp.repeat(jnp.exp(steps), shape[axis_at] // parts).reshape((-1,) + (1,) * (len(shape) - axis_at - 1))

    gain = one(*cuts[0])
    for cut in cuts[1:]:
        gain = gain * one(*cut)
    return gain


def bell_draw(rng, extent, scale, most, cuts=(), kind=jnp.bfloat16):
    level = block_levels(rng, extent, cuts, -0.22, 0.18) if cuts else 1.0
    values = jax.random.normal(rng, extent, jnp.float32) * scale * level
    return jnp.minimum(jnp.maximum(values, -most), most).astype(kind)


def setup_inputs(seed: int = 0, part: int = 0) -> dict:
    streams_of = jax.random.split(jax.random.key(seed), 14)
    part_splits = jax.random.split(jax.random.fold_in(streams_of[13], part), 14)
    return {
        "stream": bell_draw(part_splits[0], (TOKENS, D), 1.0, 6.0, ((0, 16), (1, 16))),
        "lengths": draw_lengths(jax.random.fold_in(jax.random.fold_in(streams_of[13], part), 71), part),
        "input_norm_gain": jnp.clip(1.0 + 0.18 * jax.random.normal(streams_of[2], (2, D), jnp.float32), 0.1, 1.9),
        "query_projection": bell_draw(streams_of[3], (2, D, KEYS), D ** -0.5, 0.09375, ((1, 16), (2, 16))),
        "key_projection": bell_draw(streams_of[4], (2, D, KEYS), D ** -0.5, 0.09375, ((1, 16), (2, 16))),
        "forget_gate_weight": bell_draw(streams_of[5], (2, D, KEYS), D ** -0.5, 0.09375, ((1, 16), (2, 16))),
        "value_projection": bell_draw(streams_of[6], (2, D, VALUES), D ** -0.5, 0.09375, ((1, 16), (2, 16))),
        "output_gate_weight": bell_draw(streams_of[7], (2, D, VALUES), D ** -0.5, 0.09375, ((1, 16), (2, 16))),
        "forget_gate_bias": jnp.clip(jax.random.uniform(streams_of[8], (2, KEYS), jnp.float32, -3.0, 3.0) * block_levels(streams_of[8], (2, KEYS), ((1, 16),), -0.4, 0.0), -3.0, 3.0),
        "extra_frame_decay": draw_extra_frame_decay(jax.random.fold_in(jax.random.fold_in(streams_of[13], part), 71), part),
        "head_norm_gain": jnp.clip(1.0 + 0.18 * jax.random.normal(streams_of[10], (2, VALUE_DIM), jnp.float32), 0.1, 1.9),
        "output_projection": bell_draw(streams_of[11], (2, VALUES, D), VALUES ** -0.5, 0.09375, ((1, 16), (2, 16))),
        "memory": bell_draw(part_splits[12], (2, BATCH, KEYS, VALUE_DIM), 1.0, 6.0, ((1, 16), (2, 16)), jnp.float32),
    }


EPS = 1e-06
TIME_CONSTANT = 16.0
HIGH = lax.Precision.HIGHEST

def recurrence(queries, keys_in, values_in, decay_logarithm, state_in):
    frames = queries.shape[1]
    totals = jnp.cumsum(decay_logarithm, axis=1)
    causal = (jnp.arange(frames)[:, None] >= jnp.arange(frames)[None, :])[None, :, :, None, None]
    spread = totals[:, :, None] - totals[:, None, :]
    decays = jnp.where(causal, jnp.exp(jnp.where(causal, spread, 0.0)), 0.0)
    scores = jnp.einsum('sihk,sijhk,sjhk->shij', queries, decays, keys_in, precision=HIGH)
    inner_part = jnp.einsum('shij,sjhv->sihv', scores, values_in, precision=HIGH)
    carried = jnp.einsum('sihk,shkv->sihv', queries * jnp.exp(totals), state_in, precision=HIGH)
    last_total = totals[:, -1]
    weighted = keys_in * jnp.exp(last_total[:, None] - totals)
    fresh_mem = jnp.exp(last_total)[..., None] * state_in + jnp.einsum('sjhk,sjhv->shkv', weighted, values_in, precision=HIGH)
    return (inner_part + carried, fresh_mem)

def split_sum(left_mat, right_mat, pieces):
    row_count = left_mat.shape[1] // pieces

    def add_piece(running, piece_idx):
        part = jnp.dot(lax.dynamic_slice_in_dim(left_mat, piece_idx * row_count, row_count, 1), lax.dynamic_slice_in_dim(right_mat, piece_idx * row_count, row_count, 0), preferred_element_type=jnp.float32)
        rounded = lax.optimization_barrier(part.astype(jnp.bfloat16))
        return (running + rounded.astype(jnp.float32), None)
    begin = jnp.zeros((left_mat.shape[0], right_mat.shape[1]), jnp.float32)
    running, _ = lax.scan(add_piece, begin, jnp.arange(pieces, dtype=jnp.int32))
    return running

def reference(stream, lengths, input_norm_gain, query_projection, key_projection, forget_gate_weight, value_projection, output_gate_weight, forget_gate_bias, extra_frame_decay, head_norm_gain, output_projection, memory):
    position = jnp.arange(BLOCK_LEN, dtype=jnp.int32)
    alive_mask = (position[None, :] < lengths[:, None]).astype(jnp.float32).reshape(TOKENS, 1)
    current = stream
    outputs = []
    for block_layer in range(2):
        residual = current.astype(jnp.float32)
        row_scale = lax.rsqrt(lax.optimization_barrier(jnp.mean(residual * residual, axis=1, keepdims=True)) + EPS)
        scaled = (residual * input_norm_gain[block_layer]).astype(jnp.bfloat16)
        queries = split_sum(scaled, query_projection[block_layer], N_DP) * row_scale * KEY_DIM ** (-0.5)
        keys_in = split_sum(scaled, key_projection[block_layer], N_DP) * row_scale * alive_mask
        forget_preactivation = split_sum(scaled, forget_gate_weight[block_layer], N_DP) * row_scale + forget_gate_bias[block_layer]
        values_in = split_sum(scaled, value_projection[block_layer], N_DP) * row_scale
        gate_pre = split_sum(scaled, output_gate_weight[block_layer], N_DP) * row_scale
        decay_logarithm = (jax.nn.log_sigmoid(forget_preactivation) / TIME_CONSTANT + extra_frame_decay[block_layer]) * alive_mask
        read_out, fresh_mem = recurrence(queries.reshape(BATCH, BLOCK_LEN, HEADS, KEY_DIM), keys_in.reshape(BATCH, BLOCK_LEN, HEADS, KEY_DIM), values_in.reshape(BATCH, BLOCK_LEN, HEADS, VALUE_DIM), decay_logarithm.reshape(BATCH, BLOCK_LEN, HEADS, KEY_DIM), memory[block_layer].reshape(BATCH, HEADS, KEY_DIM, VALUE_DIM))
        normed = read_out * lax.rsqrt(lax.optimization_barrier(jnp.mean(read_out * read_out, axis=3, keepdims=True)) + EPS) * head_norm_gain[block_layer]
        gated = (normed.reshape(TOKENS, VALUES) * jax.nn.silu(gate_pre) * alive_mask).astype(jnp.bfloat16)
        mixer_out = split_sum(gated, output_projection[block_layer], N_TP).astype(jnp.bfloat16)
        current = (residual + mixer_out.astype(jnp.float32)).astype(jnp.bfloat16)
        outputs.append(fresh_mem.reshape(BATCH, KEYS, VALUE_DIM))
    return (current, jnp.stack(outputs))
```

```python
import jax
import jax.numpy as jnp
from jax import lax
from jax.sharding import Mesh
from jax.sharding import PartitionSpec as P

D = 4096
KEY_DIM = 256
VALUE_DIM = 512
BLOCK_LEN = 16

EPS = 1e-06
TIME_CONSTANT = 16.0

ALONG_TP = ("a", "b")
ALONG_X = ("b", "c")


def exchange(array, axes):
    return lax.all_to_all(array, axes, 0, 0, tiled=True)


def to_all(array, axes):
    length = lax.axis_size(axes)
    return exchange(jnp.broadcast_to(array[None], (length, *array.shape)), axes)


def other(array, axis):
    return lax.ppermute(array, axis, [(0, 1), (1, 0)])


def pick(array, index, dim):
    return lax.dynamic_index_in_dim(array, index, dim, keepdims=False)


def ordered(own, theirs, spot, dim):
    return jnp.where(
        spot == 0, jnp.concatenate([own, theirs], dim), jnp.concatenate([theirs, own], dim)
    )


def three_terms(value):
    high = lax.reduce_precision(value, 8, 7)
    rest = value - high
    middle = lax.reduce_precision(rest, 8, 7)
    return [part.astype(jnp.bfloat16) for part in (high, middle, rest - middle)]


def local(
    stream,
    lengths,
    input_norm_gain,
    query_projection,
    key_projection,
    forget_gate_weight,
    value_projection,
    output_gate_weight,
    forget_gate_bias,
    extra_frame_decay,
    head_norm_gain,
    output_projection,
    memory,
):
    f32, bf16 = jnp.float32, jnp.bfloat16
    tall, wide = lax.axis_size("a"), lax.axis_size("c")
    a, b, k = lax.axis_index("a"), lax.axis_index("b"), lax.axis_index("k")
    frames, features = stream.shape
    keys = query_projection.shape[2]
    values = value_projection.shape[2]
    layers = memory.shape[0]

    gathered = to_all(stream, ALONG_TP).reshape(tall, 2, frames, features)
    x_own = pick(gathered, k, 1)
    x_other = other(pick(gathered, 1 - k, 1), "k")
    x = jnp.where(k == 0, jnp.stack([x_own, x_other], 1), jnp.stack([x_other, x_own], 1))

    gains = input_norm_gain[:, None]
    gains = ordered(gains, other(gains, "k"), k, 1)
    weights = [
        jnp.concatenate(
            [
                query_projection[n],
                key_projection[n],
                forget_gate_weight[n],
                value_projection[n],
                output_gate_weight[n],
            ],
            1,
        )
        for n in range(layers)
    ]
    weights = [ordered(w, other(w, "k"), k, 0) for w in weights]
    out_weights = ordered(output_projection[0], other(output_projection[0], "k"), k, 1)

    decay = extra_frame_decay.reshape(layers, 2, BLOCK_LEN, keys)
    decay_own = pick(decay, b, 1)
    decay = ordered(decay_own, other(pick(decay, 1 - b, 1), "b"), b, 2)
    bias = ordered(forget_gate_bias, other(forget_gate_bias, "b"), b, 1)
    state_own = pick(memory, b, 1)
    state_next = pick(memory, 1 - b, 1)
    state_other = other(state_next.astype(bf16), "b")
    position = jnp.arange(BLOCK_LEN, dtype=jnp.int32)
    alive = (position < pick(lengths, b, 0)).astype(f32)[:, None]
    causal = position[:, None] >= position[None, :]

    outputs = []
    for n in range(layers):
        wide_x = x.astype(f32)
        scaled = (wide_x * gains[n][None, :, None, :]).astype(bf16)
        scaled = jnp.swapaxes(scaled, 1, 2).reshape(tall * frames, 2 * features)
        power = jnp.sum(wide_x * wide_x, axis=(1, 3)).reshape(tall * frames, 1)
        partial = jnp.dot(scaled, weights[n], preferred_element_type=f32).astype(bf16)
        extra = three_terms(power)
        pad = jnp.zeros((tall * frames, 128 - len(extra)), bf16)
        sent = jnp.concatenate([partial, *extra, pad], 1)
        columns = sent.shape[1]
        sent = sent.reshape(tall, 2, BLOCK_LEN, columns).swapaxes(0, 1)
        got = exchange(sent.reshape(2 * tall, BLOCK_LEN, columns), ALONG_X)
        got = got.reshape(2, wide, BLOCK_LEN, columns).astype(f32).sum(axis=1)
        base = 3 * keys + 2 * values
        power = got[0, :, base : base + 1] + got[0, :, base + 1 : base + 2] + got[0, :, base + 2 : base + 3]
        got = got[:, :, :base] * lax.rsqrt(power / D + EPS)
        both = lambda low, high: jnp.concatenate([got[0, :, low:high], got[1, :, low:high]], 1)
        queries = both(0, keys) * KEY_DIM ** (-0.5)
        keys_in = both(keys, 2 * keys) * alive
        forget = both(2 * keys, 3 * keys) + bias[n]
        values_in = both(3 * keys, 3 * keys + values)
        gate = both(3 * keys + values, base)
        log_decay = (jax.nn.log_sigmoid(forget) / TIME_CONSTANT + decay[n]) * alive

        totals = jnp.cumsum(log_decay, axis=0)
        spread = totals[:, None] - totals[None, :]
        decays = jnp.where(causal[..., None], jnp.exp(jnp.where(causal[..., None], spread, 0.0)), 0.0)
        scores = jnp.einsum("ik,ijk,jk->ij", queries, decays, keys_in)
        carried = (queries * jnp.exp(totals)).reshape(BLOCK_LEN, 2, keys)
        read = (
            jnp.dot(scores, values_in)
            + jnp.dot(pick(carried, b, 1), state_own[n])
            + jnp.dot(pick(carried, 1 - b, 1).astype(bf16), state_other[n], preferred_element_type=f32)
        )
        normed = read * lax.rsqrt(jnp.mean(read * read, axis=1, keepdims=True) + EPS) * head_norm_gain[n]
        gated = (normed * jax.nn.silu(gate) * alive).astype(bf16)
        halves = gated.reshape(BLOCK_LEN, 2, values).swapaxes(0, 1)
        sent = jnp.broadcast_to(halves[:, None], (2, wide, BLOCK_LEN, values))
        got = exchange(sent.reshape(2 * wide, BLOCK_LEN, values), ALONG_X)

        last = totals[-1:]
        weighted = (keys_in * jnp.exp(last - totals)).reshape(BLOCK_LEN, 2, keys)
        kept = jnp.exp(last).reshape(2, keys)
        fresh_own = pick(kept, b, 0)[:, None] * state_own[n] + jnp.einsum(
            "jk,jv->kv", pick(weighted, b, 1), values_in
        )
        note = jnp.concatenate(
            [
                pick(weighted, 1 - b, 1),
                values_in,
                jnp.broadcast_to(pick(kept, 1 - b, 0)[None], (BLOCK_LEN, keys)),
            ],
            1,
        )
        note = other(note, "b")
        fresh_next = note[0, keys + 2 * values :][:, None] * state_next[n] + jnp.einsum(
            "jk,jv->kv", note[:, :keys], note[:, keys : keys + 2 * values]
        )
        outputs.append(
            jnp.where(b == 0, jnp.stack([fresh_own, fresh_next]), jnp.stack([fresh_next, fresh_own]))
        )

        if n + 1 < layers:
            partial = jnp.dot(
                got.reshape(2 * wide * BLOCK_LEN, values), out_weights, preferred_element_type=f32
            ).astype(bf16)
            partial = partial.reshape(2, wide, BLOCK_LEN, 2, features).transpose(1, 3, 0, 2, 4)
            residual = pick(pick(x, a, 0), b, 0)
        else:
            got = ordered(got[None], other(got, "k")[None], k, 0)
            partial = jnp.dot(
                got.reshape(4 * wide * BLOCK_LEN, values),
                output_projection[n],
                preferred_element_type=f32,
            ).astype(bf16)
            partial = partial.reshape(2, 2, wide, BLOCK_LEN, features).transpose(2, 0, 1, 3, 4)
            here = pick(x, a, 0)
            residual = jnp.where(b == k, pick(here, k, 0), other(pick(here, 1 - k, 0), "k"))
        arrived = exchange(partial.reshape(2 * wide, frames, features), ALONG_TP)
        mixer_out = arrived.astype(f32).sum(axis=0).astype(bf16)
        current = (residual.astype(f32) + mixer_out.astype(f32)).astype(bf16)
        if n + 1 < layers:
            x = to_all(current, ALONG_TP).reshape(tall, 2, frames, features)
    return current, jnp.stack(outputs)


def solution(mesh):
    grp, tp, dp = (mesh.shape[name] for name in ("grp", "tp", "dp"))
    fine = Mesh(mesh.devices.reshape(grp, tp // 2, 2, dp // 2, 2), ("grp", "a", "b", "c", "k"))
    tp, dp = ("a", "b"), ("c", "k")
    group_tp, group_dp = ("grp", *tp), ("grp", *dp)
    placed = (
        P(group_tp, dp),
        P(group_dp),
        P(None, dp),
        P(None, dp, tp),
        P(None, dp, tp),
        P(None, dp, tp),
        P(None, dp, tp),
        P(None, dp, tp),
        P(None, tp),
        P(None, group_dp, tp),
        P(),
        P(None, tp, dp),
        P(None, group_dp, tp, None),
    )
    return jax.shard_map(
        local,
        mesh=fine,
        in_specs=placed,
        out_specs=(P(group_tp, dp), P(None, group_dp, tp, None)),
        check_vma=False,
    )
```

```python
import functools

import jax
import jax.numpy as jnp
from jax import lax
from jax.experimental import pallas as pl
from jax.experimental.pallas import tpu as pltpu
from jax.sharding import Mesh
from jax.sharding import PartitionSpec as P

D = 4096
KEY_DIM = 256
VALUE_DIM = 512
BLOCK_LEN = 16

EPS = 1e-06
TIME_CONSTANT = 16.0

ALONG_TP = ("a", "b")
ALONG_X = ("b", "c")


def exchange(array, axes):
    return lax.all_to_all(array, axes, 0, 0, tiled=True)


def to_all(array, axes):
    length = lax.axis_size(axes)
    return exchange(jnp.broadcast_to(array[None], (length, *array.shape)), axes)


def other(array, axis):
    return lax.ppermute(array, axis, [(0, 1), (1, 0)])


def pick(array, index, dim):
    return lax.dynamic_index_in_dim(array, index, dim, keepdims=False)


def ordered(own, theirs, spot, dim):
    return jnp.where(
        spot == 0, jnp.concatenate([own, theirs], dim), jnp.concatenate([theirs, own], dim)
    )


LANES = 128
F32, BF16 = jnp.float32, jnp.bfloat16
EACH_ROW = (((1,), (1,)), ((), ()))
EACH_COLUMN = (((0,), (0,)), ((), ()))


def dot(left, right, dims=(((1,), (0,)), ((), ()))):
    return lax.dot_general(left, right, dims, preferred_element_type=F32)


def kernel(body, outs, *args):
    vmem = pl.BlockSpec(memory_space=pltpu.VMEM)
    return pl.pallas_call(
        body,
        out_shape=jax.tree.map(lambda out: jax.ShapeDtypeStruct(*out), outs, is_leaf=lambda x: isinstance(x[1], type)),
        in_specs=[vmem] * len(args),
        out_specs=jax.tree.map(lambda out: vmem, outs, is_leaf=lambda x: isinstance(x[1], type)),
    )(*args)


def copies_body(in_ref, out_ref):
    value = in_ref[...]
    for spot in range(out_ref.shape[0]):
        out_ref[spot] = value


def project_body(n, x_ref, mine_ref, theirs_ref, gain_ref, gain_next_ref, out_ref):
    k = lax.axis_index("k")
    tall, _, frames, features = x_ref.shape
    wide = out_ref.shape[0] // 2
    tiles = out_ref.shape[1] // BLOCK_LEN
    columns = tiles * LANES
    ones = jnp.ones((8, features), BF16)
    total, power = 0.0, 0.0
    for half, w_ref, g_ref in ((k, mine_ref, gain_ref), (1 - k, theirs_ref, gain_next_ref)):
        x = x_ref[:, half].reshape(tall * frames, features).astype(F32)
        scaled = (x * g_ref[n : n + 1, :]).astype(BF16)
        total = total + dot(scaled, w_ref[:, n * columns : (n + 1) * columns])
        square = x * x
        high = square.astype(BF16)
        low = (square - high.astype(F32)).astype(BF16)
        power = power + dot(ones, high, EACH_ROW) + dot(ones, low, EACH_ROW)
    total = total.astype(BF16)
    high = power.astype(BF16).astype(F32)
    middle = (power - high).astype(BF16).astype(F32)
    low = power - high - middle
    row = lax.broadcasted_iota(jnp.int32, power.shape, 0)
    terms = jnp.where(row == 0, high, jnp.where(row == 1, middle, jnp.where(row == 2, low, 0.0)))
    terms = terms.astype(BF16)
    for spot in range(2 * wide):
        j, c = divmod(spot, wide)
        start = c * frames + j * BLOCK_LEN
        for tile in range(tiles):
            out_ref[spot, tile * BLOCK_LEN : (tile + 1) * BLOCK_LEN, :] = total[
                start : start + BLOCK_LEN, tile * LANES : (tile + 1) * LANES
            ]
        lane = start // LANES * LANES
        out_ref[spot, tiles * BLOCK_LEN :, :] = terms[:, lane : lane + LANES]


def recur_body(n, got_ref, state_ref, state_next_ref, small_ref, gain_ref, out_ref, mine_ref, note_ref):
    b, c = lax.axis_index("b"), lax.axis_index("c")
    wide = got_ref.shape[1]
    frames = 2 * BLOCK_LEN
    summed = []
    for half in range(2):
        value = got_ref[half, 0].astype(F32)
        for spot in range(1, wide):
            value = value + got_ref[half, spot].astype(F32)
        summed.append(value)
    tiles = got_ref.shape[2] // BLOCK_LEN
    power = jnp.sum(summed[0][tiles * BLOCK_LEN :], axis=0, keepdims=True)
    row = lax.broadcasted_iota(jnp.int32, (BLOCK_LEN, LANES), 0)
    lane = lax.broadcasted_iota(jnp.int32, (BLOCK_LEN, LANES), 1)
    first = lax.rem(c * frames, LANES) + b * BLOCK_LEN
    power = jnp.sum(jnp.where(lane == row + first, power, 0.0), axis=1, keepdims=True)
    scale = lax.rsqrt(power / D + EPS)

    def tile(half, spot):
        return summed[half][spot * BLOCK_LEN : (spot + 1) * BLOCK_LEN] * scale

    alive = small_ref[n, 3 * BLOCK_LEN :]
    queries, keys, totals = [], [], []
    for half in range(2):
        queries.append(tile(half, 0) * KEY_DIM ** (-0.5))
        keys.append(tile(half, 1) * alive)
        forget = tile(half, 2) + small_ref[n, 2 * BLOCK_LEN + half : 2 * BLOCK_LEN + half + 1]
        log_gate = jnp.minimum(forget, 0.0) - jnp.log1p(jnp.exp(-jnp.abs(forget)))
        total = (log_gate / TIME_CONSTANT + small_ref[n, half * BLOCK_LEN : (half + 1) * BLOCK_LEN]) * alive
        step = 1
        while step < BLOCK_LEN:
            total = total + jnp.where(row >= step, pltpu.roll(total, step, 0), 0.0)
            step *= 2
        totals.append(total)
    value_tiles = [tile(half, spot) for half in range(2) for spot in (3, 4)]
    values = jnp.concatenate(value_tiles, 1)
    gate = jnp.concatenate([tile(half, spot) for half in range(2) for spot in (5, 6)], 1)

    carried = [queries[half] * jnp.exp(totals[half]) for half in range(2)]
    read = dot(jnp.where(b == 0, carried[0], carried[1]).astype(BF16), state_ref[n])
    read = read + dot(jnp.where(b == 0, carried[1], carried[0]).astype(BF16), state_next_ref[n])
    for spot in range(BLOCK_LEN):
        score = 0.0
        for half in range(2):
            spread = totals[half] - totals[half][spot : spot + 1]
            decay = jnp.exp(jnp.where(row >= spot, spread, 0.0))
            score = score + queries[half] * decay * keys[half][spot : spot + 1]
        score = jnp.sum(jnp.where(row >= spot, score, 0.0), axis=1, keepdims=True)
        read = read + score * values[spot : spot + 1]

    mean = jnp.mean(read * read, axis=1, keepdims=True)
    normed = read * lax.rsqrt(mean + EPS) * gain_ref[n : n + 1, :]
    gated = normed * (gate / (1.0 + jnp.exp(-gate))) * alive[:, :1]
    gated = gated.astype(BF16)
    width = out_ref.shape[2]
    for spot in range(2 * wide):
        half = spot // wide
        out_ref[spot] = gated[:, half * width : (half + 1) * width]

    weighted, kept = [], []
    for half in range(2):
        last = totals[half][BLOCK_LEN - 1 :]
        weighted.append(keys[half] * jnp.exp(last - totals[half]))
        kept.append(jnp.broadcast_to(jnp.exp(last), (BLOCK_LEN, LANES)))
    for ref, test in ((mine_ref, b == 0), (note_ref, b != 0)):
        parts = [jnp.where(test, *weighted), *value_tiles, jnp.where(test, *kept)]
        for spot, part in enumerate(parts):
            ref[spot * BLOCK_LEN : (spot + 1) * BLOCK_LEN] = part


def output_body(at, turns, left_refs, right_refs, out_ref):
    k = lax.axis_index("k")
    wide = out_ref.shape[0] // 2
    for half, left_ref, right_ref in ((k, left_refs[0], right_refs[0]), (1 - k, left_refs[1], right_refs[1])):
        width = out_ref.shape[2]
        left = left_ref[...].reshape(2 * wide * BLOCK_LEN, left_ref.shape[2])
        partial = dot(left, right_ref[:, at : at + width]).astype(BF16)
        for spot in range(2 * wide):
            j, c = divmod(spot, wide)
            out_ref[2 * c + half, j * BLOCK_LEN : (j + 1) * BLOCK_LEN, :] = partial[
                spot * BLOCK_LEN : (spot + 1) * BLOCK_LEN
            ]


def output_same_frames_body(at, left_ref, mine_ref, theirs_ref, out_ref):
    output_body(at, None, (left_ref, left_ref), (mine_ref, theirs_ref), out_ref)


def output_same_features_body(left_ref, left_next_ref, right_ref, out_ref):
    output_body(0, None, (left_ref, left_next_ref), (right_ref, right_ref), out_ref)


def add_up(ref):
    value = ref[0].astype(F32)
    for spot in range(1, ref.shape[0]):
        value = value + ref[spot].astype(F32)
    return value.astype(BF16).astype(F32)


def next_stream_body(got_ref, x_ref, out_ref):
    a, b = lax.axis_index("a"), lax.axis_index("b")
    value = (x_ref[a, b].astype(F32) + add_up(got_ref)).astype(BF16)
    for spot in range(out_ref.shape[0]):
        out_ref[spot] = value


def last_stream_body(got_ref, x_ref, next_ref, out_ref):
    a, b, k = (lax.axis_index(name) for name in "abk")
    residual = jnp.where(b == k, x_ref[a, k].astype(F32), next_ref[...].astype(F32))
    out_ref[...] = (residual + add_up(got_ref)).astype(BF16)


def memory_body(memory_ref, mine_refs, theirs_ref, out_ref):
    b = lax.axis_index("b")
    keys = memory_ref.shape[2]
    row = lax.broadcasted_iota(jnp.int32, (keys, LANES), 0)
    lane = lax.broadcasted_iota(jnp.int32, (keys, LANES), 1)
    for n in range(memory_ref.shape[0]):
        for j, note in ((b, mine_refs[n][...]), (1 - b, theirs_ref[n])):
            parts = [note[at : at + BLOCK_LEN] for at in range(0, note.shape[0], BLOCK_LEN)]
            kept = jnp.sum(jnp.where(row == lane, parts[-1][:1], 0.0), axis=1, keepdims=True)
            values = jnp.concatenate(parts[1:-1], 1).astype(BF16)
            out_ref[n, j] = kept * memory_ref[n, j] + dot(parts[0].astype(BF16), values, EACH_COLUMN)


def memory_two_body(memory_ref, mine_ref, mine_next_ref, theirs_ref, out_ref):
    memory_body(memory_ref, (mine_ref, mine_next_ref), theirs_ref, out_ref)


def local(
    stream,
    lengths,
    input_norm_gain,
    query_projection,
    key_projection,
    forget_gate_weight,
    value_projection,
    output_gate_weight,
    forget_gate_bias,
    extra_frame_decay,
    head_norm_gain,
    output_projection,
    memory,
):
    tall, wide = lax.axis_size("a"), lax.axis_size("c")
    b, k = lax.axis_index("b"), lax.axis_index("k")
    frames, features = stream.shape
    keys = query_projection.shape[2]
    values = value_projection.shape[2]
    layers = memory.shape[0]
    columns = 3 * keys + 2 * values

    sent = kernel(copies_body, ((2 * tall, frames, features), BF16), stream)
    gathered = exchange(sent, ALONG_TP).reshape(tall, 2, frames, features)

    weights = []
    for n in range(layers):
        weights += [
            query_projection[n],
            key_projection[n],
            forget_gate_weight[n],
            value_projection[n],
            output_gate_weight[n],
        ]
    mine = jnp.concatenate([*weights, output_projection[0]], 1)
    theirs = other(mine, "k")
    gain_next = other(input_norm_gain, "k")

    decay = extra_frame_decay.reshape(layers, 2, BLOCK_LEN, keys)
    bias = forget_gate_bias[:, None]
    small_next = other(jnp.concatenate([pick(decay, 1 - b, 1), bias], 1), "b")
    decay = ordered(pick(decay, b, 1), small_next[:, :BLOCK_LEN], b, 1)
    bias = ordered(bias, small_next[:, BLOCK_LEN:], b, 1)
    alive = (jnp.arange(BLOCK_LEN, dtype=jnp.int32) < pick(lengths, b, 0)).astype(F32)
    alive = jnp.broadcast_to(alive[None, :, None], (layers, BLOCK_LEN, keys))
    pad = jnp.zeros((layers, BLOCK_LEN - 2, keys), F32)
    small = jnp.concatenate([decay, bias, pad, alive], 1)
    state = pick(memory, b, 1).astype(BF16)
    state_next = other(pick(memory, 1 - b, 1).astype(BF16), "b")

    gathered, theirs, gain_next, small, state, state_next = lax.optimization_barrier(
        (gathered, theirs, gain_next, small, state, state_next)
    )
    x_own = pick(gathered, k, 1)
    x_other = other(pick(gathered, 1 - k, 1), "k")
    x = jnp.where(k == 0, jnp.stack([x_own, x_other], 1), jnp.stack([x_other, x_own], 1))

    mines, notes = [], []
    for n in range(layers):
        rows = columns // LANES * BLOCK_LEN + 8
        sent = kernel(
            functools.partial(project_body, n),
            ((2 * wide, rows, LANES), BF16),
            x,
            mine,
            theirs,
            input_norm_gain,
            gain_next,
        )
        got = exchange(sent, ALONG_X).reshape(2, wide, rows, LANES)
        note_shape = (6 * BLOCK_LEN, LANES)
        sent, own_note, note = kernel(
            functools.partial(recur_body, n),
            [((2 * wide, BLOCK_LEN, values), BF16), (note_shape, F32), (note_shape, F32)],
            got,
            state,
            state_next,
            small,
            head_norm_gain,
        )
        mines.append(own_note)
        notes.append(note)
        got = exchange(sent, ALONG_X)
        if n + 1 < layers:
            sent = kernel(
                functools.partial(output_same_frames_body, layers * columns),
                ((2 * tall, frames, features), BF16),
                got,
                mine,
                theirs,
            )
            sent = kernel(next_stream_body, ((2 * tall, frames, features), BF16), exchange(sent, ALONG_TP), x)
            x = exchange(sent, ALONG_TP).reshape(tall, 2, frames, features)
        else:
            here = pick(pick(x, lax.axis_index("a"), 0), 1 - k, 0).reshape(2, BLOCK_LEN, features)
            theirs_got = other(jnp.concatenate([got, here], 0), "k")
            sent = kernel(
                output_same_features_body,
                ((2 * tall, frames, features), BF16),
                got,
                theirs_got[: 2 * wide],
                output_projection[n],
            )
            notes, sent = lax.optimization_barrier((notes, sent))
            theirs_note = other(jnp.stack(notes), "b")
            current = kernel(
                last_stream_body,
                (stream.shape, BF16),
                exchange(sent, ALONG_TP),
                x,
                theirs_got[2 * wide :].reshape(frames, features),
            )
            fresh = kernel(memory_two_body, (memory.shape, F32), memory, *mines, theirs_note)
    return current, fresh


def solution(mesh):
    grp, tp, dp = (mesh.shape[name] for name in ("grp", "tp", "dp"))
    fine = Mesh(mesh.devices.reshape(grp, tp // 2, 2, dp // 2, 2), ("grp", "a", "b", "c", "k"))
    tp, dp = ("a", "b"), ("c", "k")
    group_tp, group_dp = ("grp", *tp), ("grp", *dp)
    placed = (
        P(group_tp, dp),
        P(group_dp),
        P(None, dp),
        P(None, dp, tp),
        P(None, dp, tp),
        P(None, dp, tp),
        P(None, dp, tp),
        P(None, dp, tp),
        P(None, tp),
        P(None, group_dp, tp),
        P(),
        P(None, tp, dp),
        P(None, group_dp, tp, None),
    )
    return jax.shard_map(
        local,
        mesh=fine,
        in_specs=placed,
        out_specs=(P(group_tp, dp), P(None, group_dp, tp, None)),
        check_vma=False,
    )
```

```python
import functools

import jax
import jax.numpy as jnp
from jax import lax
from jax.experimental import pallas as pl
from jax.experimental.pallas import tpu as pltpu
from jax.sharding import Mesh
from jax.sharding import PartitionSpec as P


D = 4096
KEY_DIM = 256
BLOCK_LEN = 16

EPS = 1e-06
TIME_CONSTANT = 16.0

ALONG_TP = ("a", "b")
ALONG_X = ("b", "c")


def exchange(array, axes):
    return lax.all_to_all(array, axes, 0, 0, tiled=True)


def other(array, axis):
    return lax.ppermute(array, axis, [(0, 1), (1, 0)])


def pick(array, index, dim):
    return lax.dynamic_index_in_dim(array, index, dim, keepdims=False)


def ordered(own, theirs, spot, dim):
    return jnp.where(
        spot == 0, jnp.concatenate([own, theirs], dim), jnp.concatenate([theirs, own], dim)
    )


LANES = 128
VMEM_LIMIT = 8 * 2**20
F32, BF16 = jnp.float32, jnp.bfloat16
EACH_ROW = (((1,), (1,)), ((), ()))
EACH_COLUMN = (((0,), (0,)), ((), ()))


def dot(left, right, dims=(((1,), (0,)), ((), ()))):
    return lax.dot_general(left, right, dims, preferred_element_type=F32)


def kernel(body, outs, *args):
    vmem = pl.BlockSpec(memory_space=pltpu.VMEM)
    return pl.pallas_call(
        body,
        out_shape=jax.tree.map(lambda out: jax.ShapeDtypeStruct(*out), outs, is_leaf=lambda x: isinstance(x[1], type)),
        in_specs=[vmem] * len(args),
        out_specs=jax.tree.map(lambda out: vmem, outs, is_leaf=lambda x: isinstance(x[1], type)),
        compiler_params=pltpu.CompilerParams(vmem_limit_bytes=VMEM_LIMIT),
    )(*args)


def copies_body(in_ref, out_ref):
    value = in_ref[...]
    for spot in range(out_ref.shape[0]):
        out_ref[spot] = value


def project_body(n, first, x_ref, x_next_ref, mine_ref, theirs_ref, gain_ref, gain_next_ref, out_ref, here_ref):
    k = lax.axis_index("k")
    tall, _, frames, features = x_ref.shape
    wide = out_ref.shape[0] // 2
    tiles = out_ref.shape[1] // BLOCK_LEN
    columns = tiles * LANES
    ones = jnp.ones((8, features), BF16)
    total, power = 0.0, 0.0
    for half, w_ref, g_ref in ((k, mine_ref, gain_ref), (1 - k, theirs_ref, gain_next_ref)):
        x = x_next_ref[...] if first and half is not k else x_ref[:, half]
        x = x.reshape(tall * frames, features).astype(F32)
        scaled = (x * g_ref[n : n + 1, :]).astype(BF16)
        total = total + dot(scaled, w_ref[:, n * columns : (n + 1) * columns])
        square = x * x
        high = square.astype(BF16)
        low = (square - high.astype(F32)).astype(BF16)
        power = power + dot(ones, high, EACH_ROW) + dot(ones, low, EACH_ROW)
    here_ref[...] = x_ref[lax.axis_index("a"), 1 - k]
    total = total.astype(BF16)
    high = power.astype(BF16).astype(F32)
    middle = (power - high).astype(BF16).astype(F32)
    low = power - high - middle
    row = lax.broadcasted_iota(jnp.int32, power.shape, 0)
    terms = jnp.where(row == 0, high, jnp.where(row == 1, middle, jnp.where(row == 2, low, 0.0)))
    terms = terms.astype(BF16)
    for spot in range(2 * wide):
        j, c = divmod(spot, wide)
        start = c * frames + j * BLOCK_LEN
        for tile in range(tiles):
            out_ref[spot, tile * BLOCK_LEN : (tile + 1) * BLOCK_LEN, :] = total[
                start : start + BLOCK_LEN, tile * LANES : (tile + 1) * LANES
            ]
        lane = start // LANES * LANES
        out_ref[spot, tiles * BLOCK_LEN :, :] = terms[:, lane : lane + LANES]


def recur_body(n, got_ref, state_ref, state_next_ref, small_ref, gain_ref, out_ref, mine_ref, note_ref):
    b, c = lax.axis_index("b"), lax.axis_index("c")
    wide = got_ref.shape[1]
    frames = 2 * BLOCK_LEN
    summed = []
    for half in range(2):
        value = got_ref[half, 0].astype(F32)
        for spot in range(1, wide):
            value = value + got_ref[half, spot].astype(F32)
        summed.append(value)
    tiles = got_ref.shape[2] // BLOCK_LEN
    power = jnp.sum(summed[0][tiles * BLOCK_LEN :], axis=0, keepdims=True)
    row = lax.broadcasted_iota(jnp.int32, (BLOCK_LEN, LANES), 0)
    lane = lax.broadcasted_iota(jnp.int32, (BLOCK_LEN, LANES), 1)
    first = lax.rem(c * frames, LANES) + b * BLOCK_LEN
    power = jnp.sum(jnp.where(lane == row + first, power, 0.0), axis=1, keepdims=True)
    scale = lax.rsqrt(power / D + EPS)

    def tile(half, spot):
        return summed[half][spot * BLOCK_LEN : (spot + 1) * BLOCK_LEN] * scale

    alive = small_ref[n, 3 * BLOCK_LEN :]
    queries, keys, totals = [], [], []
    for half in range(2):
        queries.append(tile(half, 0) * KEY_DIM ** (-0.5))
        keys.append(tile(half, 1) * alive)
        forget = tile(half, 2) + small_ref[n, 2 * BLOCK_LEN + half : 2 * BLOCK_LEN + half + 1]
        log_gate = jnp.minimum(forget, 0.0) - jnp.log1p(jnp.exp(-jnp.abs(forget)))
        total = (log_gate / TIME_CONSTANT + small_ref[n, half * BLOCK_LEN : (half + 1) * BLOCK_LEN]) * alive
        step = 1
        while step < BLOCK_LEN:
            total = total + jnp.where(row >= step, pltpu.roll(total, step, 0), 0.0)
            step *= 2
        totals.append(total)
    value_tiles = [tile(half, spot) for half in range(2) for spot in (3, 4)]
    values = jnp.concatenate(value_tiles, 1)
    gate = jnp.concatenate([tile(half, spot) for half in range(2) for spot in (5, 6)], 1)

    carried = [queries[half] * jnp.exp(totals[half]) for half in range(2)]
    read = dot(jnp.where(b == 0, carried[0], carried[1]).astype(BF16), state_ref[n])
    read = read + dot(jnp.where(b == 0, carried[1], carried[0]).astype(BF16), state_next_ref[n])
    for spot in range(BLOCK_LEN):
        score = 0.0
        for half in range(2):
            spread = totals[half] - totals[half][spot : spot + 1]
            decay = jnp.exp(jnp.where(row >= spot, spread, 0.0))
            score = score + queries[half] * decay * keys[half][spot : spot + 1]
        score = jnp.sum(jnp.where(row >= spot, score, 0.0), axis=1, keepdims=True)
        read = read + score * values[spot : spot + 1]

    mean = jnp.mean(read * read, axis=1, keepdims=True)
    normed = read * lax.rsqrt(mean + EPS) * gain_ref[n : n + 1, :]
    gated = normed * (gate / (1.0 + jnp.exp(-gate))) * alive[:, :1]
    gated = gated.astype(BF16)
    width = out_ref.shape[2]
    for spot in range(2 * wide):
        half = spot // wide
        out_ref[spot] = gated[:, half * width : (half + 1) * width]

    weighted, kept = [], []
    for half in range(2):
        last = totals[half][BLOCK_LEN - 1 :]
        weighted.append(keys[half] * jnp.exp(last - totals[half]))
        kept.append(jnp.broadcast_to(jnp.exp(last), (BLOCK_LEN, LANES)))
    for ref, test in ((mine_ref, b == 0), (note_ref, b != 0)):
        parts = [jnp.where(test, *weighted), *value_tiles, jnp.where(test, *kept)]
        for spot, part in enumerate(parts):
            ref[spot * BLOCK_LEN : (spot + 1) * BLOCK_LEN] = part


def output_body(at, left_refs, right_refs, out_ref):
    k = lax.axis_index("k")
    wide = out_ref.shape[0] // 2
    for half, left_ref, right_ref in ((k, left_refs[0], right_refs[0]), (1 - k, left_refs[1], right_refs[1])):
        width = out_ref.shape[2]
        left = left_ref[...].reshape(2 * wide * BLOCK_LEN, left_ref.shape[2])
        partial = dot(left, right_ref[:, at : at + width]).astype(BF16)
        for spot in range(2 * wide):
            j, c = divmod(spot, wide)
            out_ref[2 * c + half, j * BLOCK_LEN : (j + 1) * BLOCK_LEN, :] = partial[
                spot * BLOCK_LEN : (spot + 1) * BLOCK_LEN
            ]


def output_same_frames_body(at, left_ref, mine_ref, theirs_ref, out_ref):
    output_body(at, (left_ref, left_ref), (mine_ref, theirs_ref), out_ref)


def output_same_features_body(left_ref, left_next_ref, right_ref, out_ref):
    output_body(0, (left_ref, left_next_ref), (right_ref, right_ref), out_ref)


def add_up(ref):
    value = ref[0].astype(F32)
    for spot in range(1, ref.shape[0]):
        value = value + ref[spot].astype(F32)
    return value.astype(BF16).astype(F32)


def next_stream_body(got_ref, x_ref, x_next_ref, out_ref):
    a, b, k = (lax.axis_index(name) for name in "abk")
    residual = jnp.where(b == k, x_ref[a, k].astype(F32), x_next_ref[a].astype(F32))
    value = (residual + add_up(got_ref)).astype(BF16)
    for spot in range(out_ref.shape[0]):
        out_ref[spot] = value


def last_stream_body(got_ref, x_ref, next_ref, out_ref):
    a, b, k = (lax.axis_index(name) for name in "abk")
    residual = jnp.where(b == k, x_ref[a, k].astype(F32), next_ref[...].astype(F32))
    out_ref[...] = (residual + add_up(got_ref)).astype(BF16)


def memory_body(memory_ref, mine_refs, theirs_ref, out_ref):
    b = lax.axis_index("b")
    keys = memory_ref.shape[2]
    row = lax.broadcasted_iota(jnp.int32, (keys, LANES), 0)
    lane = lax.broadcasted_iota(jnp.int32, (keys, LANES), 1)
    for n in range(memory_ref.shape[0]):
        for j, note in ((b, mine_refs[n][...]), (1 - b, theirs_ref[n])):
            parts = [note[at : at + BLOCK_LEN] for at in range(0, note.shape[0], BLOCK_LEN)]
            kept = jnp.sum(jnp.where(row == lane, parts[-1][:1], 0.0), axis=1, keepdims=True)
            values = jnp.concatenate(parts[1:-1], 1).astype(BF16)
            out_ref[n, j] = kept * memory_ref[n, j] + dot(parts[0].astype(BF16), values, EACH_COLUMN)


def memory_two_body(memory_ref, mine_ref, mine_next_ref, theirs_ref, out_ref):
    memory_body(memory_ref, (mine_ref, mine_next_ref), theirs_ref, out_ref)


def local(
    stream,
    lengths,
    input_norm_gain,
    query_projection,
    key_projection,
    forget_gate_weight,
    value_projection,
    output_gate_weight,
    forget_gate_bias,
    extra_frame_decay,
    head_norm_gain,
    output_projection,
    memory,
):
    tall, wide = lax.axis_size("a"), lax.axis_size("c")
    b, k = lax.axis_index("b"), lax.axis_index("k")
    frames, features = stream.shape
    keys = query_projection.shape[2]
    values = value_projection.shape[2]
    layers = memory.shape[0]
    columns = 3 * keys + 2 * values

    sent = kernel(copies_body, ((2 * tall, frames, features), BF16), stream)
    sent, *weights_in = lax.optimization_barrier(
        (
            sent,
            query_projection,
            key_projection,
            forget_gate_weight,
            value_projection,
            output_gate_weight,
            output_projection,
        )
    )
    gathered = exchange(sent, ALONG_TP).reshape(tall, 2, frames, features)

    weights = []
    for n in range(layers):
        weights += [weight[n] for weight in weights_in[:-1]]
    mine = jnp.concatenate([*weights, weights_in[-1][0]], 1)
    theirs = other(mine, "k")
    gain_next = other(input_norm_gain, "k")

    decay = extra_frame_decay.reshape(layers, 2, BLOCK_LEN, keys)
    bias = forget_gate_bias[:, None]
    small_next = other(jnp.concatenate([pick(decay, 1 - b, 1), bias], 1), "b")
    decay = ordered(pick(decay, b, 1), small_next[:, :BLOCK_LEN], b, 1)
    bias = ordered(bias, small_next[:, BLOCK_LEN:], b, 1)
    alive = (jnp.arange(BLOCK_LEN, dtype=jnp.int32) < pick(lengths, b, 0)).astype(F32)
    alive = jnp.broadcast_to(alive[None, :, None], (layers, BLOCK_LEN, keys))
    pad = jnp.zeros((layers, BLOCK_LEN - 2, keys), F32)
    small = jnp.concatenate([decay, bias, pad, alive], 1)
    state = pick(memory, b, 1).astype(BF16)
    state_next = other(pick(memory, 1 - b, 1).astype(BF16), "b")

    gathered, theirs, gain_next, small, state, state_next = lax.optimization_barrier(
        (gathered, theirs, gain_next, small, state, state_next)
    )
    x, x_next = gathered, other(pick(gathered, 1 - k, 1), "k")

    mines, notes = [], []
    for n in range(layers):
        rows = columns // LANES * BLOCK_LEN + 8
        sent, here = kernel(
            functools.partial(project_body, n, n == 0),
            [((2 * wide, rows, LANES), BF16), ((frames, features), BF16)],
            x,
            x_next,
            mine,
            theirs,
            input_norm_gain,
            gain_next,
        )
        got = exchange(sent, ALONG_X).reshape(2, wide, rows, LANES)
        note_shape = (6 * BLOCK_LEN, LANES)
        sent, own_note, note = kernel(
            functools.partial(recur_body, n),
            [((2 * wide, BLOCK_LEN, values), BF16), (note_shape, F32), (note_shape, F32)],
            got,
            state,
            state_next,
            small,
            head_norm_gain,
        )
        mines.append(own_note)
        notes.append(note)
        got = exchange(sent, ALONG_X)
        if n + 1 < layers:
            sent = kernel(
                functools.partial(output_same_frames_body, layers * columns),
                ((2 * tall, frames, features), BF16),
                got,
                mine,
                theirs,
            )
            sent = kernel(next_stream_body, ((2 * tall, frames, features), BF16), exchange(sent, ALONG_TP), x, x_next)
            x = exchange(sent, ALONG_TP).reshape(tall, 2, frames, features)
        else:
            theirs_got = other(jnp.concatenate([got, here.reshape(2, BLOCK_LEN, features)], 0), "k")
            sent = kernel(
                output_same_features_body,
                ((2 * tall, frames, features), BF16),
                got,
                theirs_got[: 2 * wide],
                output_projection[n],
            )
            notes, sent = lax.optimization_barrier((notes, sent))
            theirs_note = other(jnp.stack(notes), "b")
            current = kernel(
                last_stream_body,
                (stream.shape, BF16),
                exchange(sent, ALONG_TP),
                x,
                theirs_got[2 * wide :].reshape(frames, features),
            )
            fresh = kernel(memory_two_body, (memory.shape, F32), memory, *mines, theirs_note)
    return current, fresh


def solution(mesh):
    grp, tp, dp = (mesh.shape[name] for name in ("grp", "tp", "dp"))
    fine = Mesh(mesh.devices.reshape(grp, tp // 2, 2, dp // 2, 2), ("grp", "a", "b", "c", "k"))
    tp, dp = ("a", "b"), ("c", "k")
    group_tp, group_dp = ("grp", *tp), ("grp", *dp)
    placed = (
        P(group_tp, dp),
        P(group_dp),
        P(None, dp),
        P(None, dp, tp),
        P(None, dp, tp),
        P(None, dp, tp),
        P(None, dp, tp),
        P(None, dp, tp),
        P(None, tp),
        P(None, group_dp, tp),
        P(),
        P(None, tp, dp),
        P(None, group_dp, tp, None),
    )

    return jax.shard_map(
        local,
        mesh=fine,
        in_specs=placed,
        out_specs=(P(group_tp, dp), P(None, group_dp, tp, None)),
        check_vma=False,
    )
```

```python
import functools

import jax
import jax.numpy as jnp
from jax import lax
from jax.experimental import pallas as pl
from jax.experimental.pallas import tpu as pltpu
from jax.sharding import Mesh
from jax.sharding import PartitionSpec as P


D = 4096
KEY_DIM = 256
VALUE_DIM = 512
BLOCK_LEN = 16

EPS = 1e-06
TIME_CONSTANT = 16.0

ALONG_TP = ("far", "near", "b")
QUAD = ("near", "b")
HEAD = ("far", "near")
ALONG_X = ("b", "c")


def exchange(array, axes):
    return lax.all_to_all(array, axes, 0, 0, tiled=True)


def other(array, axis):
    return lax.ppermute(array, axis, [(0, 1), (1, 0)])


LANES = 128
VMEM_LIMIT = 8 * 2**20
F32, BF16 = jnp.float32, jnp.bfloat16
EACH_ROW = (((1,), (1,)), ((), ()))
EACH_COLUMN = (((0,), (0,)), ((), ()))


def dot(left, right, dims=(((1,), (0,)), ((), ()))):
    return lax.dot_general(left, right, dims, preferred_element_type=F32)


def kernel(body, outs, *args):
    vmem = pl.BlockSpec(memory_space=pltpu.VMEM)
    several = isinstance(outs, list)
    shapes = [jax.ShapeDtypeStruct(*out) for out in (outs if several else [outs])]
    return pl.pallas_call(
        body,
        out_shape=shapes if several else shapes[0],
        in_specs=[vmem] * len(args),
        out_specs=[vmem] * len(shapes) if several else vmem,
        compiler_params=pltpu.CompilerParams(vmem_limit_bytes=VMEM_LIMIT),
    )(*args)


def three_terms(value):
    high = value.astype(BF16).astype(F32)
    middle = (value - high).astype(BF16).astype(F32)
    return high, middle, value - high - middle


def head_index():
    return lax.axis_index("far") * lax.axis_size("near") + lax.axis_index("near")


def write_copies(out_ref, value):
    for spot in range(out_ref.shape[0]):
        out_ref[spot] = value


def copies_body(in_ref, out_ref):
    write_copies(out_ref, in_ref[...])


def pack_state_body(memory_ref, decay_ref, bias_ref, out_ref):
    j = 1 - lax.axis_index("b")
    keys = memory_ref.shape[2]
    for n in range(memory_ref.shape[0]):
        out_ref[n, :keys] = memory_ref[n, j].astype(BF16)
        bias = jnp.broadcast_to(bias_ref[n : n + 1, :], (BLOCK_LEN, keys))
        for at, value in ((keys, decay_ref[n, j]), (keys + BLOCK_LEN, bias)):
            for spot, term in enumerate(three_terms(value)):
                out_ref[n, at : at + BLOCK_LEN, spot * keys : (spot + 1) * keys] = term.astype(BF16)


def project_body(n, first, x_ref, x_next_ref, mine_ref, theirs_ref, out_ref, here_ref):
    k = lax.axis_index("k")
    tall, _, frames, features = x_ref.shape
    wide = out_ref.shape[0] // 2
    tiles = out_ref.shape[1] // BLOCK_LEN
    columns = tiles * LANES
    ones = jnp.ones((8, features), BF16)
    total, power = 0.0, 0.0
    for half, w_ref in ((k, mine_ref), (1 - k, theirs_ref)):
        x = x_next_ref[...] if first and half is not k else x_ref[:, half]
        x = x.reshape(tall * frames, features)
        total = total + dot(x, w_ref[:, n * columns : (n + 1) * columns])
        square = x.astype(F32) * x.astype(F32)
        high = square.astype(BF16)
        low = (square - high.astype(F32)).astype(BF16)
        power = power + dot(ones, high, EACH_ROW) + dot(ones, low, EACH_ROW)
    here_ref[...] = x_ref[head_index(), 1 - k]
    total = total.astype(BF16)
    high, middle, low = three_terms(power)
    row = lax.broadcasted_iota(jnp.int32, power.shape, 0)
    terms = jnp.where(row == 0, high, jnp.where(row == 1, middle, jnp.where(row == 2, low, 0.0)))
    terms = terms.astype(BF16)
    for spot in range(2 * wide):
        j, c = divmod(spot, wide)
        start = c * frames + j * BLOCK_LEN
        for tile in range(tiles):
            out_ref[spot, tile * BLOCK_LEN : (tile + 1) * BLOCK_LEN, :] = total[
                start : start + BLOCK_LEN, tile * LANES : (tile + 1) * LANES
            ]
        lane = start // LANES * LANES
        out_ref[spot, tiles * BLOCK_LEN :, :] = terms[:, lane : lane + LANES]


def recur_body(
    n,
    got_ref,
    memory_ref,
    packet_ref,
    decay_ref,
    bias_ref,
    lengths_ref,
    gain_ref,
    out_ref,
    mine_ref,
    note_ref,
):
    b, c = lax.axis_index("b"), lax.axis_index("c")
    wide = got_ref.shape[1]
    frames = 2 * BLOCK_LEN
    summed = []
    for half in range(2):
        value = got_ref[half, 0].astype(F32)
        for spot in range(1, wide):
            value = value + got_ref[half, spot].astype(F32)
        summed.append(value)
    tiles = got_ref.shape[2] // BLOCK_LEN
    power = jnp.sum(summed[0][tiles * BLOCK_LEN :], axis=0, keepdims=True)
    row = lax.broadcasted_iota(jnp.int32, (BLOCK_LEN, LANES), 0)
    lane = lax.broadcasted_iota(jnp.int32, (BLOCK_LEN, LANES), 1)
    first = lax.rem(c * frames, LANES) + b * BLOCK_LEN
    power = jnp.sum(jnp.where(lane == row + first, power, 0.0), axis=1, keepdims=True)
    scale = lax.rsqrt(power / D + EPS)

    def tile(half, spot):
        return summed[half][spot * BLOCK_LEN : (spot + 1) * BLOCK_LEN] * scale

    def unpacked(at):
        block = packet_ref[n, at : at + BLOCK_LEN, : 3 * LANES].astype(F32)
        return block[:, :LANES] + block[:, LANES : 2 * LANES] + block[:, 2 * LANES :]

    own_keys = memory_ref.shape[2]
    length = lengths_ref[...].astype(F32)
    here = lax.broadcasted_iota(jnp.int32, length.shape, 1) == b
    length = jnp.sum(jnp.where(here, length, 0.0), axis=1, keepdims=True)
    alive = jnp.where(row.astype(F32) < length, 1.0, 0.0)
    extra = (decay_ref[n, b], unpacked(own_keys))
    bias = (jnp.broadcast_to(bias_ref[n : n + 1, :], extra[0].shape), unpacked(own_keys + BLOCK_LEN))
    queries, keys, totals = [], [], []
    for half in range(2):
        queries.append(tile(half, 0) * KEY_DIM ** (-0.5))
        keys.append(tile(half, 1) * alive)
        forget = tile(half, 2) + jnp.where(b == half, *bias)
        log_gate = jnp.minimum(forget, 0.0) - jnp.log1p(jnp.exp(-jnp.abs(forget)))
        total = (log_gate / TIME_CONSTANT + jnp.where(b == half, *extra)) * alive
        step = 1
        while step < BLOCK_LEN:
            total = total + jnp.where(row >= step, pltpu.roll(total, step, 0), 0.0)
            step *= 2
        totals.append(total)
    value_tiles = [tile(half, spot) for half in range(2) for spot in (3, 4)]
    values = jnp.concatenate(value_tiles, 1)
    gate = jnp.concatenate([tile(half, spot) for half in range(2) for spot in (5, 6)], 1)

    carried = [queries[half] * jnp.exp(totals[half]) for half in range(2)]
    read = dot(jnp.where(b == 0, carried[0], carried[1]).astype(BF16), memory_ref[n, b].astype(BF16))
    read = read + dot(jnp.where(b == 0, carried[1], carried[0]).astype(BF16), packet_ref[n, :own_keys])
    for spot in range(BLOCK_LEN):
        score = 0.0
        for half in range(2):
            spread = totals[half] - totals[half][spot : spot + 1]
            decay = jnp.exp(jnp.where(row >= spot, spread, 0.0))
            score = score + queries[half] * decay * keys[half][spot : spot + 1]
        score = jnp.sum(jnp.where(row >= spot, score, 0.0), axis=1, keepdims=True)
        read = read + score * values[spot : spot + 1]

    mean = jnp.mean(read * read, axis=1, keepdims=True)
    normed = read * lax.rsqrt(mean + EPS) * gain_ref[n : n + 1, :]
    gated = normed * (gate / (1.0 + jnp.exp(-gate))) * alive[:, :1]
    gated = gated.astype(BF16)
    width = out_ref.shape[2]
    for spot in range(2 * wide):
        half = spot // wide
        out_ref[spot] = gated[:, half * width : (half + 1) * width]

    weighted, kept = [], []
    for half in range(2):
        last = totals[half][BLOCK_LEN - 1 :]
        weighted.append(keys[half] * jnp.exp(last - totals[half]))
        kept.append(jnp.broadcast_to(jnp.exp(last), (BLOCK_LEN, LANES)))
    for ref, test in ((mine_ref, b == 0), (note_ref, b != 0)):
        parts = [jnp.where(test, *weighted), *value_tiles, jnp.where(test, *kept)]
        for spot, part in enumerate(parts):
            ref[spot * BLOCK_LEN : (spot + 1) * BLOCK_LEN] = part


def output_body(at, left_refs, right_refs, out_ref):
    k = lax.axis_index("k")
    wide = out_ref.shape[0] // 2
    for half, left_ref, right_ref in ((k, left_refs[0], right_refs[0]), (1 - k, left_refs[1], right_refs[1])):
        width = out_ref.shape[2]
        left = left_ref[...].reshape(2 * wide * BLOCK_LEN, left_ref.shape[2])
        partial = dot(left, right_ref[:, at : at + width]).astype(BF16)
        for spot in range(2 * wide):
            j, c = divmod(spot, wide)
            out_ref[2 * c + half, j * BLOCK_LEN : (j + 1) * BLOCK_LEN, :] = partial[
                spot * BLOCK_LEN : (spot + 1) * BLOCK_LEN
            ]


def output_same_frames_body(at, left_ref, mine_ref, theirs_ref, out_ref):
    output_body(at, (left_ref, left_ref), (mine_ref, theirs_ref), out_ref)


def output_same_features_body(left_ref, left_next_ref, right_ref, out_ref):
    output_body(0, (left_ref, left_next_ref), (right_ref, right_ref), out_ref)


def add_up(ref):
    value = ref[0].astype(F32)
    for spot in range(1, ref.shape[0]):
        value = value + ref[spot].astype(F32)
    return value.astype(BF16).astype(F32)


def quad_sum_body(got_ref, out_ref):
    write_copies(out_ref, add_up(got_ref).astype(BF16))


def next_stream_body(got_ref, x_ref, x_next_ref, out_ref):
    b, k = lax.axis_index("b"), lax.axis_index("k")
    frames = x_ref.shape[2]
    blocks = got_ref.shape[1] // frames
    first = (2 * lax.axis_index("near") + b) * (blocks // 2)
    summed = add_up(got_ref)
    for block in range(blocks):
        c, half = first + block // 2, block % 2
        residual = jnp.where(k == half, x_ref[c, k].astype(F32), x_next_ref[c].astype(F32))
        rows = slice(block * frames, (block + 1) * frames)
        value = (residual + summed[rows]).astype(BF16)
        for spot in range(out_ref.shape[0]):
            out_ref[spot, rows, :] = value


def last_stream_body(got_ref, x_ref, next_ref, out_ref):
    a, b, k = head_index(), lax.axis_index("b"), lax.axis_index("k")
    residual = jnp.where(b == k, x_ref[a, k].astype(F32), next_ref[...].astype(F32))
    out_ref[...] = (residual + add_up(got_ref)).astype(BF16)


def memory_body(memory_ref, mine_refs, theirs_ref, out_ref):
    b = lax.axis_index("b")
    keys = memory_ref.shape[2]
    row = lax.broadcasted_iota(jnp.int32, (keys, LANES), 0)
    lane = lax.broadcasted_iota(jnp.int32, (keys, LANES), 1)
    for n in range(memory_ref.shape[0]):
        for j, note in ((b, mine_refs[n][...]), (1 - b, theirs_ref[n])):
            parts = [note[at : at + BLOCK_LEN] for at in range(0, note.shape[0], BLOCK_LEN)]
            kept = jnp.sum(jnp.where(row == lane, parts[-1][:1], 0.0), axis=1, keepdims=True)
            values = jnp.concatenate(parts[1:-1], 1).astype(BF16)
            out_ref[n, j] = kept * memory_ref[n, j] + dot(parts[0].astype(BF16), values, EACH_COLUMN)


def memory_two_body(memory_ref, mine_ref, mine_next_ref, theirs_ref, out_ref):
    memory_body(memory_ref, (mine_ref, mine_next_ref), theirs_ref, out_ref)


def local(
    stream,
    lengths,
    input_norm_gain,
    query_projection,
    key_projection,
    forget_gate_weight,
    value_projection,
    output_gate_weight,
    forget_gate_bias,
    extra_frame_decay,
    head_norm_gain,
    output_projection,
    memory,
):
    quads, quad = lax.axis_size("far"), lax.axis_size(QUAD)
    tall, wide = lax.axis_size(HEAD), lax.axis_size("c")
    k = lax.axis_index("k")
    frames, features = stream.shape
    keys = query_projection.shape[2]
    values = value_projection.shape[2]
    layers = memory.shape[0]
    columns = 3 * keys + 2 * values
    decay = extra_frame_decay.reshape(layers, 2, BLOCK_LEN, keys)

    sent = kernel(copies_body, ((2 * tall, frames, features), BF16), stream)
    x = exchange(sent, ALONG_TP).reshape(tall, 2, frames, features)
    packet = kernel(pack_state_body, ((layers, keys + 2 * BLOCK_LEN, VALUE_DIM), BF16), memory, decay, forget_gate_bias)
    weights = [
        query_projection,
        key_projection,
        forget_gate_weight,
        value_projection,
        output_gate_weight,
    ]
    weights = [
        (weight[n].astype(F32) * input_norm_gain[n][:, None]).astype(BF16)
        for n in range(layers)
        for weight in weights
    ]
    mine = jnp.concatenate([*weights, output_projection[0]], 1)
    theirs = other(mine, "k")
    packet = other(packet, "b")
    x, theirs, packet = lax.optimization_barrier((x, theirs, packet))
    x_next = other(lax.dynamic_index_in_dim(x, 1 - k, 1, keepdims=False), "k")

    mines, notes = [], []
    for n in range(layers):
        rows = columns // LANES * BLOCK_LEN + 8
        sent, here = kernel(
            functools.partial(project_body, n, n == 0),
            [((2 * wide, rows, LANES), BF16), ((frames, features), BF16)],
            x,
            x_next,
            mine,
            theirs,
        )
        got = exchange(sent, ALONG_X).reshape(2, wide, rows, LANES)
        note_shape = (6 * BLOCK_LEN, LANES)
        sent, own_note, note = kernel(
            functools.partial(recur_body, n),
            [((2 * wide, BLOCK_LEN, values), BF16), (note_shape, F32), (note_shape, F32)],
            got,
            memory,
            packet,
            decay,
            forget_gate_bias,
            lengths[None],
            head_norm_gain,
        )
        mines.append(own_note)
        notes.append(note)
        got = exchange(sent, ALONG_X)
        if n + 1 < layers:
            sent = kernel(
                functools.partial(output_same_frames_body, layers * columns),
                ((2 * tall, frames, features), BF16),
                got,
                mine,
                theirs,
            )
            shape = (frames * 2 * tall // quad, features)
            got = exchange(sent.reshape(quad, *shape), QUAD)
            sent = kernel(quad_sum_body, ((quads, *shape), BF16), got)
            sent = kernel(next_stream_body, ((quad, *shape), BF16), exchange(sent, "far"), x, x_next)
            x = exchange(sent, QUAD).reshape(tall, 2, frames, features)
        else:
            theirs_got = other(jnp.concatenate([got, here.reshape(2, BLOCK_LEN, features)], 0), "k")
            sent = kernel(
                output_same_features_body,
                ((2 * tall, frames, features), BF16),
                got,
                theirs_got[: 2 * wide],
                output_projection[n],
            )
            notes, sent = lax.optimization_barrier((notes, sent))
            theirs_note = other(jnp.stack(notes), "b")
            current = kernel(
                last_stream_body,
                (stream.shape, BF16),
                exchange(sent, ALONG_TP),
                x,
                theirs_got[2 * wide :].reshape(frames, features),
            )
            fresh = kernel(memory_two_body, (memory.shape, F32), memory, *mines, theirs_note)
    return current, fresh


def solution(mesh):
    grp, tp, dp = (mesh.shape[name] for name in ("grp", "tp", "dp"))
    fine = Mesh(
        mesh.devices.reshape(grp, tp // 4, 2, 2, dp // 2, 2), ("grp", *ALONG_TP, "c", "k")
    )
    tp, dp = ALONG_TP, ("c", "k")
    group_tp, group_dp = ("grp", *tp), ("grp", *dp)
    placed = (
        P(group_tp, dp),
        P(group_dp),
        P(None, dp),
        P(None, dp, tp),
        P(None, dp, tp),
        P(None, dp, tp),
        P(None, dp, tp),
        P(None, dp, tp),
        P(None, tp),
        P(None, group_dp, tp),
        P(),
        P(None, tp, dp),
        P(None, group_dp, tp, None),
    )

    return jax.shard_map(
        local,
        mesh=fine,
        in_specs=placed,
        out_specs=(P(group_tp, dp), P(None, group_dp, tp, None)),
        check_vma=False,
    )
```

```python
import functools

import jax
import jax.numpy as jnp
from jax import lax
from jax.experimental import pallas as pl
from jax.experimental.pallas import tpu as pltpu
from jax.sharding import Mesh
from jax.sharding import PartitionSpec as P


D = 4096
KEY_DIM = 256
VALUE_DIM = 512
BLOCK_LEN = 16

EPS = 1e-06
TIME_CONSTANT = 16.0

ALONG_TP = ("far", "near", "b")
QUAD = ("near", "b")
HEAD = ("far", "near")
ALONG_X = ("b", "c")


def exchange(array, axes):
    return lax.all_to_all(array, axes, 0, 0, tiled=True)


def other(array, axis):
    return lax.ppermute(array, axis, [(0, 1), (1, 0)])


LANES = 128
VMEM_LIMIT = 8 * 2**20
F32, BF16 = jnp.float32, jnp.bfloat16
EACH_ROW = (((1,), (1,)), ((), ()))
EACH_COLUMN = (((0,), (0,)), ((), ()))


def dot(left, right, dims=(((1,), (0,)), ((), ()))):
    return lax.dot_general(left, right, dims, preferred_element_type=F32)


def kernel(body, outs, *args):
    vmem = pl.BlockSpec(memory_space=pltpu.VMEM)
    several = isinstance(outs, list)
    shapes = [jax.ShapeDtypeStruct(*out) for out in (outs if several else [outs])]
    return pl.pallas_call(
        body,
        out_shape=shapes if several else shapes[0],
        in_specs=[vmem] * len(args),
        out_specs=[vmem] * len(shapes) if several else vmem,
        compiler_params=pltpu.CompilerParams(vmem_limit_bytes=VMEM_LIMIT),
    )(*args)


def three_terms(value):
    high = value.astype(BF16).astype(F32)
    middle = (value - high).astype(BF16).astype(F32)
    return high, middle, value - high - middle


def head_index():
    return lax.axis_index("far") * lax.axis_size("near") + lax.axis_index("near")


def write_copies(out_ref, value):
    for spot in range(out_ref.shape[0]):
        out_ref[spot] = value


def copies_body(in_ref, out_ref):
    write_copies(out_ref, in_ref[...])


def pack_state_body(memory_ref, decay_ref, bias_ref, out_ref):
    j = 1 - lax.axis_index("b")
    keys = memory_ref.shape[2]
    for n in range(memory_ref.shape[0]):
        out_ref[n, :keys] = memory_ref[n, j].astype(BF16)
        bias = jnp.broadcast_to(bias_ref[n : n + 1, :], (BLOCK_LEN, keys))
        for at, value in ((keys, decay_ref[n, j]), (keys + BLOCK_LEN, bias)):
            for spot, term in enumerate(three_terms(value)):
                out_ref[n, at : at + BLOCK_LEN, spot * keys : (spot + 1) * keys] = term.astype(BF16)


def project_body(n, first, x_ref, x_next_ref, mine_ref, theirs_ref, out_ref, here_ref):
    k = lax.axis_index("k")
    tall, _, frames, features = x_ref.shape
    wide = out_ref.shape[0] // 2
    tiles = out_ref.shape[1] // BLOCK_LEN
    columns = tiles * LANES
    ones = jnp.ones((8, features), BF16)
    total, power = 0.0, 0.0
    for half, w_ref in ((k, mine_ref), (1 - k, theirs_ref)):
        x = x_next_ref[...] if first and half is not k else x_ref[:, half]
        x = x.reshape(tall * frames, features)
        total = total + dot(x, w_ref[:, n * columns : (n + 1) * columns])
        square = x.astype(F32) * x.astype(F32)
        high = square.astype(BF16)
        low = (square - high.astype(F32)).astype(BF16)
        power = power + dot(ones, high, EACH_ROW) + dot(ones, low, EACH_ROW)
    here_ref[...] = x_ref[head_index(), 1 - k]
    total = total.astype(BF16)
    high, middle, low = three_terms(power)
    row = lax.broadcasted_iota(jnp.int32, power.shape, 0)
    terms = jnp.where(row == 0, high, jnp.where(row == 1, middle, jnp.where(row == 2, low, 0.0)))
    terms = terms.astype(BF16)
    for spot in range(2 * wide):
        j, c = divmod(spot, wide)
        start = c * frames + j * BLOCK_LEN
        for tile in range(tiles):
            out_ref[spot, tile * BLOCK_LEN : (tile + 1) * BLOCK_LEN, :] = total[
                start : start + BLOCK_LEN, tile * LANES : (tile + 1) * LANES
            ]
        lane = start // LANES * LANES
        out_ref[spot, tiles * BLOCK_LEN :, :] = terms[:, lane : lane + LANES]


def chips_sum_body(got_ref, out_ref):
    for half in range(2):
        value = got_ref[half, 0].astype(F32)
        for spot in range(1, got_ref.shape[1]):
            value = value + got_ref[half, spot].astype(F32)
        out_ref[half] = value


def recur_body(
    n,
    got_ref,
    memory_ref,
    packet_ref,
    decay_ref,
    bias_ref,
    lengths_ref,
    gain_ref,
    out_ref,
    mine_ref,
    note_ref,
):
    b, c = lax.axis_index("b"), lax.axis_index("c")
    wide = out_ref.shape[0] // 2
    frames = 2 * BLOCK_LEN
    summed = [got_ref[half] for half in range(2)]
    tiles = got_ref.shape[1] // BLOCK_LEN
    power = jnp.sum(summed[0][tiles * BLOCK_LEN :], axis=0, keepdims=True)
    row = lax.broadcasted_iota(jnp.int32, (BLOCK_LEN, LANES), 0)
    lane = lax.broadcasted_iota(jnp.int32, (BLOCK_LEN, LANES), 1)
    first = lax.rem(c * frames, LANES) + b * BLOCK_LEN
    power = jnp.sum(jnp.where(lane == row + first, power, 0.0), axis=1, keepdims=True)
    scale = lax.rsqrt(power / D + EPS)

    def tile(half, spot):
        return summed[half][spot * BLOCK_LEN : (spot + 1) * BLOCK_LEN] * scale

    def unpacked(at):
        block = packet_ref[n, at : at + BLOCK_LEN, : 3 * LANES].astype(F32)
        return block[:, :LANES] + block[:, LANES : 2 * LANES] + block[:, 2 * LANES :]

    own_keys = memory_ref.shape[2]
    length = lengths_ref[...].astype(F32)
    here = lax.broadcasted_iota(jnp.int32, length.shape, 1) == b
    length = jnp.sum(jnp.where(here, length, 0.0), axis=1, keepdims=True)
    alive = jnp.where(row.astype(F32) < length, 1.0, 0.0)
    extra = (decay_ref[n, b], unpacked(own_keys))
    bias = (jnp.broadcast_to(bias_ref[n : n + 1, :], extra[0].shape), unpacked(own_keys + BLOCK_LEN))
    queries, keys, totals = [], [], []
    for half in range(2):
        queries.append(tile(half, 0) * KEY_DIM ** (-0.5))
        keys.append(tile(half, 1) * alive)
        forget = tile(half, 2) + jnp.where(b == half, *bias)
        log_gate = jnp.minimum(forget, 0.0) - jnp.log1p(jnp.exp(-jnp.abs(forget)))
        total = (log_gate / TIME_CONSTANT + jnp.where(b == half, *extra)) * alive
        step = 1
        while step < BLOCK_LEN:
            total = total + jnp.where(row >= step, pltpu.roll(total, step, 0), 0.0)
            step *= 2
        totals.append(total)
    value_tiles = [tile(half, spot) for half in range(2) for spot in (3, 4)]
    values = jnp.concatenate(value_tiles, 1)
    gate = jnp.concatenate([tile(half, spot) for half in range(2) for spot in (5, 6)], 1)

    carried = [queries[half] * jnp.exp(totals[half]) for half in range(2)]
    read = dot(jnp.where(b == 0, carried[0], carried[1]).astype(BF16), memory_ref[n, b].astype(BF16))
    read = read + dot(jnp.where(b == 0, carried[1], carried[0]).astype(BF16), packet_ref[n, :own_keys])
    for spot in range(BLOCK_LEN):
        score = 0.0
        for half in range(2):
            spread = totals[half] - totals[half][spot : spot + 1]
            decay = jnp.exp(jnp.where(row >= spot, spread, 0.0))
            score = score + queries[half] * decay * keys[half][spot : spot + 1]
        score = jnp.sum(jnp.where(row >= spot, score, 0.0), axis=1, keepdims=True)
        read = read + score * values[spot : spot + 1]

    mean = jnp.mean(read * read, axis=1, keepdims=True)
    normed = read * lax.rsqrt(mean + EPS) * gain_ref[n : n + 1, :]
    gated = normed * (gate / (1.0 + jnp.exp(-gate))) * alive[:, :1]
    gated = gated.astype(BF16)
    width = out_ref.shape[2]
    for spot in range(2 * wide):
        half = spot // wide
        out_ref[spot] = gated[:, half * width : (half + 1) * width]

    weighted, kept = [], []
    for half in range(2):
        last = totals[half][BLOCK_LEN - 1 :]
        weighted.append(keys[half] * jnp.exp(last - totals[half]))
        kept.append(jnp.broadcast_to(jnp.exp(last), (BLOCK_LEN, LANES)))
    for ref, test in ((mine_ref, b == 0), (note_ref, b != 0)):
        parts = [jnp.where(test, *weighted), *value_tiles, jnp.where(test, *kept)]
        for spot, part in enumerate(parts):
            ref[spot * BLOCK_LEN : (spot + 1) * BLOCK_LEN] = part


def output_body(at, left_refs, right_refs, out_ref):
    k = lax.axis_index("k")
    wide = out_ref.shape[0] // 2
    for half, left_ref, right_ref in ((k, left_refs[0], right_refs[0]), (1 - k, left_refs[1], right_refs[1])):
        width = out_ref.shape[2]
        left = left_ref[...].reshape(2 * wide * BLOCK_LEN, left_ref.shape[2])
        partial = dot(left, right_ref[:, at : at + width]).astype(BF16)
        for spot in range(2 * wide):
            j, c = divmod(spot, wide)
            out_ref[2 * c + half, j * BLOCK_LEN : (j + 1) * BLOCK_LEN, :] = partial[
                spot * BLOCK_LEN : (spot + 1) * BLOCK_LEN
            ]


def output_same_frames_body(at, left_ref, mine_ref, theirs_ref, out_ref):
    output_body(at, (left_ref, left_ref), (mine_ref, theirs_ref), out_ref)


def output_same_features_body(left_ref, left_next_ref, right_ref, out_ref):
    output_body(0, (left_ref, left_next_ref), (right_ref, right_ref), out_ref)


def add_up(ref):
    value = ref[0].astype(F32)
    for spot in range(1, ref.shape[0]):
        value = value + ref[spot].astype(F32)
    return value.astype(BF16).astype(F32)


def quad_sum_body(got_ref, out_ref):
    write_copies(out_ref, add_up(got_ref).astype(BF16))


def next_stream_body(got_ref, x_ref, x_next_ref, out_ref):
    b, k = lax.axis_index("b"), lax.axis_index("k")
    frames = x_ref.shape[2]
    blocks = got_ref.shape[1] // frames
    first = (2 * lax.axis_index("near") + b) * (blocks // 2)
    summed = add_up(got_ref)
    for block in range(blocks):
        c, half = first + block // 2, block % 2
        residual = jnp.where(k == half, x_ref[c, k].astype(F32), x_next_ref[c].astype(F32))
        rows = slice(block * frames, (block + 1) * frames)
        value = (residual + summed[rows]).astype(BF16)
        for spot in range(out_ref.shape[0]):
            out_ref[spot, rows, :] = value


def last_stream_body(got_ref, x_ref, next_ref, out_ref):
    a, b, k = head_index(), lax.axis_index("b"), lax.axis_index("k")
    residual = jnp.where(b == k, x_ref[a, k].astype(F32), next_ref[...].astype(F32))
    out_ref[...] = (residual + add_up(got_ref)).astype(BF16)


def memory_body(memory_ref, mine_refs, theirs_ref, out_ref):
    b = lax.axis_index("b")
    keys = memory_ref.shape[2]
    row = lax.broadcasted_iota(jnp.int32, (keys, LANES), 0)
    lane = lax.broadcasted_iota(jnp.int32, (keys, LANES), 1)
    for n in range(memory_ref.shape[0]):
        for j, note in ((b, mine_refs[n][...]), (1 - b, theirs_ref[n])):
            parts = [note[at : at + BLOCK_LEN] for at in range(0, note.shape[0], BLOCK_LEN)]
            kept = jnp.sum(jnp.where(row == lane, parts[-1][:1], 0.0), axis=1, keepdims=True)
            values = jnp.concatenate(parts[1:-1], 1).astype(BF16)
            out_ref[n, j] = kept * memory_ref[n, j] + dot(parts[0].astype(BF16), values, EACH_COLUMN)


def memory_two_body(memory_ref, mine_ref, mine_next_ref, theirs_ref, out_ref):
    memory_body(memory_ref, (mine_ref, mine_next_ref), theirs_ref, out_ref)


def local(
    stream,
    lengths,
    input_norm_gain,
    query_projection,
    key_projection,
    forget_gate_weight,
    value_projection,
    output_gate_weight,
    forget_gate_bias,
    extra_frame_decay,
    head_norm_gain,
    output_projection,
    memory,
):
    quads, quad = lax.axis_size("far"), lax.axis_size(QUAD)
    tall, wide = lax.axis_size(HEAD), lax.axis_size("c")
    k = lax.axis_index("k")
    frames, features = stream.shape
    keys = query_projection.shape[2]
    values = value_projection.shape[2]
    layers = memory.shape[0]
    columns = 3 * keys + 2 * values
    decay = extra_frame_decay.reshape(layers, 2, BLOCK_LEN, keys)

    sent = kernel(copies_body, ((2 * tall, frames, features), BF16), stream)
    x = exchange(sent, ALONG_TP).reshape(tall, 2, frames, features)
    packet = kernel(pack_state_body, ((layers, keys + 2 * BLOCK_LEN, VALUE_DIM), BF16), memory, decay, forget_gate_bias)
    weights = [
        query_projection,
        key_projection,
        forget_gate_weight,
        value_projection,
        output_gate_weight,
    ]
    weights = [
        (weight[n].astype(F32) * input_norm_gain[n][:, None]).astype(BF16)
        for n in range(layers)
        for weight in weights
    ]
    mine = jnp.concatenate([*weights, output_projection[0]], 1)
    theirs = other(mine, "k")
    packet = other(packet, "b")
    x, theirs = lax.optimization_barrier((x, theirs))
    x_next = other(lax.dynamic_index_in_dim(x, 1 - k, 1, keepdims=False), "k")

    mines, notes = [], []
    for n in range(layers):
        rows = columns // LANES * BLOCK_LEN + 8
        sent, here = kernel(
            functools.partial(project_body, n, n == 0),
            [((2 * wide, rows, LANES), BF16), ((frames, features), BF16)],
            x,
            x_next,
            mine,
            theirs,
        )
        got = exchange(sent, ALONG_X).reshape(2, wide, rows, LANES)
        got = kernel(chips_sum_body, ((2, rows, LANES), F32), got)
        note_shape = (6 * BLOCK_LEN, LANES)
        sent, own_note, note = kernel(
            functools.partial(recur_body, n),
            [((2 * wide, BLOCK_LEN, values), BF16), (note_shape, F32), (note_shape, F32)],
            got,
            memory,
            packet,
            decay,
            forget_gate_bias,
            lengths[None],
            head_norm_gain,
        )
        mines.append(own_note)
        notes.append(note)
        got = exchange(sent, ALONG_X)
        if n + 1 < layers:
            sent = kernel(
                functools.partial(output_same_frames_body, layers * columns),
                ((2 * tall, frames, features), BF16),
                got,
                mine,
                theirs,
            )
            shape = (frames * 2 * tall // quad, features)
            got = exchange(sent.reshape(quad, *shape), QUAD)
            sent = kernel(quad_sum_body, ((quads, *shape), BF16), got)
            sent = kernel(next_stream_body, ((quad, *shape), BF16), exchange(sent, "far"), x, x_next)
            x = exchange(sent, QUAD).reshape(tall, 2, frames, features)
        else:
            theirs_got = other(jnp.concatenate([got, here.reshape(2, BLOCK_LEN, features)], 0), "k")
            sent = kernel(
                output_same_features_body,
                ((2 * tall, frames, features), BF16),
                got,
                theirs_got[: 2 * wide],
                output_projection[n],
            )
            notes, sent = lax.optimization_barrier((notes, sent))
            theirs_note = other(jnp.stack(notes), "b")
            current = kernel(
                last_stream_body,
                (stream.shape, BF16),
                exchange(sent, ALONG_TP),
                x,
                theirs_got[2 * wide :].reshape(frames, features),
            )
            fresh = kernel(memory_two_body, (memory.shape, F32), memory, *mines, theirs_note)
    return current, fresh


def solution(mesh):
    grp, tp, dp = (mesh.shape[name] for name in ("grp", "tp", "dp"))
    fine = Mesh(
        mesh.devices.reshape(grp, tp // 4, 2, 2, dp // 2, 2), ("grp", *ALONG_TP, "c", "k")
    )
    tp, dp = ALONG_TP, ("c", "k")
    group_tp, group_dp = ("grp", *tp), ("grp", *dp)
    placed = (
        P(group_tp, dp),
        P(group_dp),
        P(None, dp),
        P(None, dp, tp),
        P(None, dp, tp),
        P(None, dp, tp),
        P(None, dp, tp),
        P(None, dp, tp),
        P(None, tp),
        P(None, group_dp, tp),
        P(),
        P(None, tp, dp),
        P(None, group_dp, tp, None),
    )

    return jax.shard_map(
        local,
        mesh=fine,
        in_specs=placed,
        out_specs=(P(group_tp, dp), P(None, group_dp, tp, None)),
        check_vma=False,
    )
```

```python
import functools

import jax
import jax.numpy as jnp
from jax import lax
from jax.experimental import pallas as pl
from jax.experimental.pallas import tpu as pltpu
from jax.sharding import Mesh
from jax.sharding import PartitionSpec as P


D = 4096
KEY_DIM = 256
VALUE_DIM = 512
BLOCK_LEN = 16

EPS = 1e-06
TIME_CONSTANT = 16.0

ALONG_TP = ("far", "near", "b")
QUAD = ("near", "b")
HEAD = ("far", "near")
ALONG_X = ("b", "c")


def exchange(array, axes):
    return lax.all_to_all(array, axes, 0, 0, tiled=True)


def other(array, axis):
    return lax.ppermute(array, axis, [(0, 1), (1, 0)])


LANES = 128
VMEM_LIMIT = 8 * 2**20
F32, BF16 = jnp.float32, jnp.bfloat16
EACH_ROW = (((1,), (1,)), ((), ()))
EACH_COLUMN = (((0,), (0,)), ((), ()))


def dot(left, right, dims=(((1,), (0,)), ((), ()))):
    return lax.dot_general(left, right, dims, preferred_element_type=F32)


def kernel(body, outs, *args):
    vmem = pl.BlockSpec(memory_space=pltpu.VMEM)
    several = isinstance(outs, list)
    shapes = [jax.ShapeDtypeStruct(*out) for out in (outs if several else [outs])]
    return pl.pallas_call(
        body,
        out_shape=shapes if several else shapes[0],
        in_specs=[vmem] * len(args),
        out_specs=[vmem] * len(shapes) if several else vmem,
        compiler_params=pltpu.CompilerParams(vmem_limit_bytes=VMEM_LIMIT),
    )(*args)


def three_terms(value):
    high = value.astype(BF16).astype(F32)
    middle = (value - high).astype(BF16).astype(F32)
    return high, middle, value - high - middle


def head_index():
    return lax.axis_index("far") * lax.axis_size("near") + lax.axis_index("near")


def write_copies(out_ref, value):
    for spot in range(out_ref.shape[0]):
        out_ref[spot] = value


def copies_body(in_ref, out_ref):
    write_copies(out_ref, in_ref[...])


def pack_state_body(memory_ref, decay_ref, bias_ref, lengths_ref, gain_ref, out_ref, alive_ref, kept_gain_ref):
    j = 1 - lax.axis_index("b")
    length = lengths_ref[...].astype(F32)
    here = lax.broadcasted_iota(jnp.int32, length.shape, 1) != j
    length = jnp.sum(jnp.where(here, length, 0.0), axis=1, keepdims=True)
    row = lax.broadcasted_iota(jnp.int32, alive_ref.shape, 0).astype(F32)
    alive_ref[...] = jnp.where(row < length, 1.0, 0.0)
    kept_gain_ref[...] = gain_ref[...]
    keys = memory_ref.shape[2]
    for n in range(memory_ref.shape[0]):
        out_ref[n, :keys] = memory_ref[n, j].astype(BF16)
        bias = jnp.broadcast_to(bias_ref[n : n + 1, :], (BLOCK_LEN, keys))
        for at, value in ((keys, decay_ref[n, j]), (keys + BLOCK_LEN, bias)):
            for spot, term in enumerate(three_terms(value)):
                out_ref[n, at : at + BLOCK_LEN, spot * keys : (spot + 1) * keys] = term.astype(BF16)


def project_body(n, first, x_ref, x_next_ref, mine_ref, theirs_ref, out_ref, here_ref=None):
    k = lax.axis_index("k")
    tall, _, frames, features = x_ref.shape
    wide = out_ref.shape[0] // 2
    tiles = out_ref.shape[1] // BLOCK_LEN
    columns = tiles * LANES
    ones = jnp.ones((8, features), BF16)
    total, power = 0.0, 0.0
    for half, w_ref in ((k, mine_ref), (1 - k, theirs_ref)):
        x = x_next_ref[...] if first and half is not k else x_ref[:, half]
        x = x.reshape(tall * frames, features)
        total = total + dot(x, w_ref[:, n * columns : (n + 1) * columns])
        square = x.astype(F32) * x.astype(F32)
        high = square.astype(BF16)
        low = (square - high.astype(F32)).astype(BF16)
        power = power + dot(ones, high, EACH_ROW) + dot(ones, low, EACH_ROW)
    if here_ref is not None:
        here_ref[...] = x_ref[head_index(), 1 - k]
    total = total.astype(BF16)
    high, middle, low = three_terms(power)
    row = lax.broadcasted_iota(jnp.int32, power.shape, 0)
    terms = jnp.where(row == 0, high, jnp.where(row == 1, middle, jnp.where(row == 2, low, 0.0)))
    terms = terms.astype(BF16)
    for spot in range(2 * wide):
        j, c = divmod(spot, wide)
        start = c * frames + j * BLOCK_LEN
        for tile in range(tiles):
            out_ref[spot, tile * BLOCK_LEN : (tile + 1) * BLOCK_LEN, :] = total[
                start : start + BLOCK_LEN, tile * LANES : (tile + 1) * LANES
            ]
        lane = start // LANES * LANES
        out_ref[spot, tiles * BLOCK_LEN :, :] = terms[:, lane : lane + LANES]


def chips_sum_body(got_ref, out_ref):
    for half in range(2):
        value = got_ref[half, 0].astype(F32)
        for spot in range(1, got_ref.shape[1]):
            value = value + got_ref[half, spot].astype(F32)
        out_ref[half] = value


def recur_body(
    n,
    got_ref,
    memory_ref,
    packet_ref,
    decay_ref,
    bias_ref,
    alive_ref,
    gain_ref,
    out_ref,
    mine_ref,
    note_ref,
):
    b, c = lax.axis_index("b"), lax.axis_index("c")
    wide = out_ref.shape[0] // 2
    frames = 2 * BLOCK_LEN
    summed = [got_ref[half] for half in range(2)]
    tiles = got_ref.shape[1] // BLOCK_LEN
    power = jnp.sum(summed[0][tiles * BLOCK_LEN :], axis=0, keepdims=True)
    row = lax.broadcasted_iota(jnp.int32, (BLOCK_LEN, LANES), 0)
    lane = lax.broadcasted_iota(jnp.int32, (BLOCK_LEN, LANES), 1)
    first = lax.rem(c * frames, LANES) + b * BLOCK_LEN
    power = jnp.sum(jnp.where(lane == row + first, power, 0.0), axis=1, keepdims=True)
    scale = lax.rsqrt(power / D + EPS)

    def tile(half, spot):
        return summed[half][spot * BLOCK_LEN : (spot + 1) * BLOCK_LEN] * scale

    def unpacked(at):
        block = packet_ref[n, at : at + BLOCK_LEN, : 3 * LANES].astype(F32)
        return block[:, :LANES] + block[:, LANES : 2 * LANES] + block[:, 2 * LANES :]

    own_keys = memory_ref.shape[2]
    alive = alive_ref[...]
    extra = (decay_ref[n, b], unpacked(own_keys))
    bias = (jnp.broadcast_to(bias_ref[n : n + 1, :], extra[0].shape), unpacked(own_keys + BLOCK_LEN))
    queries, keys, totals = [], [], []
    for half in range(2):
        queries.append(tile(half, 0) * KEY_DIM ** (-0.5))
        keys.append(tile(half, 1) * alive)
        forget = tile(half, 2) + jnp.where(b == half, *bias)
        log_gate = jnp.minimum(forget, 0.0) - jnp.log1p(jnp.exp(-jnp.abs(forget)))
        total = (log_gate / TIME_CONSTANT + jnp.where(b == half, *extra)) * alive
        step = 1
        while step < BLOCK_LEN:
            total = total + jnp.where(row >= step, pltpu.roll(total, step, 0), 0.0)
            step *= 2
        totals.append(total)
    value_tiles = [tile(half, spot) for half in range(2) for spot in (3, 4)]
    values = jnp.concatenate(value_tiles, 1)
    gate = jnp.concatenate([tile(half, spot) for half in range(2) for spot in (5, 6)], 1)

    carried = [queries[half] * jnp.exp(totals[half]) for half in range(2)]
    read = dot(jnp.where(b == 0, carried[0], carried[1]).astype(BF16), memory_ref[n, b].astype(BF16))
    read = read + dot(jnp.where(b == 0, carried[1], carried[0]).astype(BF16), packet_ref[n, :own_keys])
    for spot in range(BLOCK_LEN):
        score = 0.0
        for half in range(2):
            spread = totals[half] - totals[half][spot : spot + 1]
            decay = jnp.exp(jnp.where(row >= spot, spread, 0.0))
            score = score + queries[half] * decay * keys[half][spot : spot + 1]
        score = jnp.sum(jnp.where(row >= spot, score, 0.0), axis=1, keepdims=True)
        read = read + score * values[spot : spot + 1]

    mean = jnp.mean(read * read, axis=1, keepdims=True)
    normed = read * lax.rsqrt(mean + EPS) * gain_ref[n : n + 1, :]
    gated = normed * (gate / (1.0 + jnp.exp(-gate))) * alive[:, :1]
    gated = gated.astype(BF16)
    width = out_ref.shape[2]
    for spot in range(2 * wide):
        half = spot // wide
        out_ref[spot] = gated[:, half * width : (half + 1) * width]

    weighted, kept = [], []
    for half in range(2):
        last = totals[half][BLOCK_LEN - 1 :]
        weighted.append(keys[half] * jnp.exp(last - totals[half]))
        kept.append(jnp.broadcast_to(jnp.exp(last), (BLOCK_LEN, LANES)))
    for ref, test in ((mine_ref, b == 0), (note_ref, b != 0)):
        parts = [jnp.where(test, *weighted), *value_tiles, jnp.where(test, *kept)]
        for spot, part in enumerate(parts):
            ref[spot * BLOCK_LEN : (spot + 1) * BLOCK_LEN] = part


def output_body(at, left_refs, right_refs, out_ref):
    k = lax.axis_index("k")
    wide = out_ref.shape[0] // 2
    for half, left_ref, right_ref in ((k, left_refs[0], right_refs[0]), (1 - k, left_refs[1], right_refs[1])):
        width = out_ref.shape[2]
        left = left_ref[...].reshape(2 * wide * BLOCK_LEN, left_ref.shape[2])
        partial = dot(left, right_ref[:, at : at + width]).astype(BF16)
        for spot in range(2 * wide):
            j, c = divmod(spot, wide)
            out_ref[2 * c + half, j * BLOCK_LEN : (j + 1) * BLOCK_LEN, :] = partial[
                spot * BLOCK_LEN : (spot + 1) * BLOCK_LEN
            ]


def output_same_frames_body(at, left_ref, mine_ref, theirs_ref, out_ref):
    output_body(at, (left_ref, left_ref), (mine_ref, theirs_ref), out_ref)


def output_same_features_body(left_ref, left_next_ref, right_ref, out_ref):
    output_body(0, (left_ref, left_next_ref), (right_ref, right_ref), out_ref)


def add_up(ref):
    value = ref[0].astype(F32)
    for spot in range(1, ref.shape[0]):
        value = value + ref[spot].astype(F32)
    return value.astype(BF16).astype(F32)


def quad_sum_body(got_ref, out_ref):
    write_copies(out_ref, add_up(got_ref).astype(BF16))


def next_stream_body(got_ref, x_ref, x_next_ref, out_ref):
    b, k = lax.axis_index("b"), lax.axis_index("k")
    frames = x_ref.shape[2]
    blocks = got_ref.shape[1] // frames
    first = (2 * lax.axis_index("near") + b) * (blocks // 2)
    summed = add_up(got_ref)
    for block in range(blocks):
        c, half = first + block // 2, block % 2
        residual = jnp.where(k == half, x_ref[c, k].astype(F32), x_next_ref[c].astype(F32))
        rows = slice(block * frames, (block + 1) * frames)
        value = (residual + summed[rows]).astype(BF16)
        for spot in range(out_ref.shape[0]):
            out_ref[spot, rows, :] = value


def last_stream_body(got_ref, x_ref, next_ref, out_ref):
    a, b, k = head_index(), lax.axis_index("b"), lax.axis_index("k")
    residual = jnp.where(b == k, x_ref[a, k].astype(F32), next_ref[...].astype(F32))
    out_ref[...] = (residual + add_up(got_ref)).astype(BF16)


def memory_body(memory_ref, mine_refs, theirs_ref, out_ref):
    b = lax.axis_index("b")
    keys = memory_ref.shape[2]
    row = lax.broadcasted_iota(jnp.int32, (keys, LANES), 0)
    lane = lax.broadcasted_iota(jnp.int32, (keys, LANES), 1)
    for n in range(memory_ref.shape[0]):
        for j, note in ((b, mine_refs[n][...]), (1 - b, theirs_ref[n])):
            parts = [note[at : at + BLOCK_LEN] for at in range(0, note.shape[0], BLOCK_LEN)]
            kept = jnp.sum(jnp.where(row == lane, parts[-1][:1], 0.0), axis=1, keepdims=True)
            values = jnp.concatenate(parts[1:-1], 1).astype(BF16)
            out_ref[n, j] = kept * memory_ref[n, j] + dot(parts[0].astype(BF16), values, EACH_COLUMN)


def memory_two_body(memory_ref, mine_ref, mine_next_ref, theirs_ref, out_ref):
    memory_body(memory_ref, (mine_ref, mine_next_ref), theirs_ref, out_ref)


def local(
    stream,
    lengths,
    input_norm_gain,
    query_projection,
    key_projection,
    forget_gate_weight,
    value_projection,
    output_gate_weight,
    forget_gate_bias,
    extra_frame_decay,
    head_norm_gain,
    output_projection,
    memory,
):
    quads, quad = lax.axis_size("far"), lax.axis_size(QUAD)
    tall, wide = lax.axis_size(HEAD), lax.axis_size("c")
    k = lax.axis_index("k")
    frames, features = stream.shape
    keys = query_projection.shape[2]
    values = value_projection.shape[2]
    layers = memory.shape[0]
    columns = 3 * keys + 2 * values
    decay = extra_frame_decay.reshape(layers, 2, BLOCK_LEN, keys)

    sent = kernel(copies_body, ((2 * tall, frames, features), BF16), stream)
    x = exchange(sent, ALONG_TP).reshape(tall, 2, frames, features)
    packet, alive, kept_gain = kernel(
        pack_state_body,
        [
            ((layers, keys + 2 * BLOCK_LEN, VALUE_DIM), BF16),
            ((BLOCK_LEN, LANES), F32),
            (head_norm_gain.shape, F32),
        ],
        memory,
        decay,
        forget_gate_bias,
        lengths[None],
        head_norm_gain,
    )
    weights = [
        query_projection,
        key_projection,
        forget_gate_weight,
        value_projection,
        output_gate_weight,
    ]
    weights = [
        (weight[n].astype(F32) * input_norm_gain[n][:, None]).astype(BF16)
        for n in range(layers)
        for weight in weights
    ]
    mine = jnp.concatenate([*weights, output_projection[0]], 1)
    theirs = other(mine, "k")
    packet = other(packet, "b")
    x, theirs = lax.optimization_barrier((x, theirs))
    x_next = other(lax.dynamic_index_in_dim(x, 1 - k, 1, keepdims=False), "k")

    mines, notes = [], []
    for n in range(layers):
        rows = columns // LANES * BLOCK_LEN + 8
        outs = [((2 * wide, rows, LANES), BF16), ((frames, features), BF16)]
        sent, *here = kernel(
            functools.partial(project_body, n, n == 0),
            outs if n + 1 == layers else outs[:1],
            x,
            x_next,
            mine,
            theirs,
        )
        got = exchange(sent, ALONG_X).reshape(2, wide, rows, LANES)
        got = kernel(chips_sum_body, ((2, rows, LANES), F32), got)
        note_shape = (6 * BLOCK_LEN, LANES)
        sent, own_note, note = kernel(
            functools.partial(recur_body, n),
            [((2 * wide, BLOCK_LEN, values), BF16), (note_shape, F32), (note_shape, F32)],
            got,
            memory,
            packet,
            decay,
            forget_gate_bias,
            alive,
            kept_gain,
        )
        mines.append(own_note)
        notes.append(note)
        got = exchange(sent, ALONG_X)
        if n + 1 < layers:
            sent = kernel(
                functools.partial(output_same_frames_body, layers * columns),
                ((2 * tall, frames, features), BF16),
                got,
                mine,
                theirs,
            )
            shape = (frames * 2 * tall // quad, features)
            got = exchange(sent.reshape(quad, *shape), QUAD)
            sent = kernel(quad_sum_body, ((quads, *shape), BF16), got)
            sent = kernel(next_stream_body, ((quad, *shape), BF16), exchange(sent, "far"), x, x_next)
            x = exchange(sent, QUAD).reshape(tall, 2, frames, features)
        else:
            theirs_got = other(jnp.concatenate([got, here[0].reshape(2, BLOCK_LEN, features)], 0), "k")
            sent = kernel(
                output_same_features_body,
                ((2 * tall, frames, features), BF16),
                got,
                theirs_got[: 2 * wide],
                output_projection[n],
            )
            notes, sent = lax.optimization_barrier((notes, sent))
            theirs_note = other(jnp.stack(notes), "b")
            current = kernel(
                last_stream_body,
                (stream.shape, BF16),
                exchange(sent, ALONG_TP),
                x,
                theirs_got[2 * wide :].reshape(frames, features),
            )
            fresh = kernel(memory_two_body, (memory.shape, F32), memory, *mines, theirs_note)
    return current, fresh


def solution(mesh):
    grp, tp, dp = (mesh.shape[name] for name in ("grp", "tp", "dp"))
    fine = Mesh(
        mesh.devices.reshape(grp, tp // 4, 2, 2, dp // 2, 2), ("grp", *ALONG_TP, "c", "k")
    )
    tp, dp = ALONG_TP, ("c", "k")
    group_tp, group_dp = ("grp", *tp), ("grp", *dp)
    placed = (
        P(group_tp, dp),
        P(group_dp),
        P(None, dp),
        P(None, dp, tp),
        P(None, dp, tp),
        P(None, dp, tp),
        P(None, dp, tp),
        P(None, dp, tp),
        P(None, tp),
        P(None, group_dp, tp),
        P(),
        P(None, tp, dp),
        P(None, group_dp, tp, None),
    )

    return jax.shard_map(
        local,
        mesh=fine,
        in_specs=placed,
        out_specs=(P(group_tp, dp), P(None, group_dp, tp, None)),
        check_vma=False,
    )
```

```python
import functools

import jax
import jax.numpy as jnp
from jax import lax
from jax.experimental import pallas as pl
from jax.experimental.pallas import tpu as pltpu
from jax.sharding import Mesh
from jax.sharding import PartitionSpec as P


D = 4096
KEY_DIM = 256
VALUE_DIM = 512
BLOCK_LEN = 16

EPS = 1e-06
TIME_CONSTANT = 16.0

ALONG_TP = ("far", "near", "b")
QUAD = ("near", "b")
HEAD = ("far", "near")
ALONG_X = ("b", "c")


def exchange(array, axes):
    return lax.all_to_all(array, axes, 0, 0, tiled=True)


def other(array, axis):
    return lax.ppermute(array, axis, [(0, 1), (1, 0)])


LANES = 128
VMEM_LIMIT = 8 * 2**20
F32, BF16 = jnp.float32, jnp.bfloat16
EACH_ROW = (((1,), (1,)), ((), ()))
EACH_COLUMN = (((0,), (0,)), ((), ()))


def dot(left, right, dims=(((1,), (0,)), ((), ()))):
    return lax.dot_general(left, right, dims, preferred_element_type=F32)


def kernel(body, outs, *args):
    vmem = pl.BlockSpec(memory_space=pltpu.VMEM)
    several = isinstance(outs, list)
    shapes = [jax.ShapeDtypeStruct(*out) for out in (outs if several else [outs])]
    return pl.pallas_call(
        body,
        out_shape=shapes if several else shapes[0],
        in_specs=[vmem] * len(args),
        out_specs=[vmem] * len(shapes) if several else vmem,
        compiler_params=pltpu.CompilerParams(vmem_limit_bytes=VMEM_LIMIT),
    )(*args)


def three_terms(value):
    high = value.astype(BF16).astype(F32)
    middle = (value - high).astype(BF16).astype(F32)
    return high, middle, value - high - middle


def head_index():
    return lax.axis_index("far") * lax.axis_size("near") + lax.axis_index("near")


def write_copies(out_ref, value):
    for spot in range(out_ref.shape[0]):
        out_ref[spot] = value


def copies_body(in_ref, out_ref):
    write_copies(out_ref, in_ref[...])


def pack_state_body(memory_ref, decay_ref, bias_ref, lengths_ref, gain_ref, out_ref, alive_ref, kept_gain_ref):
    j = 1 - lax.axis_index("b")
    length = lengths_ref[...].astype(F32)
    here = lax.broadcasted_iota(jnp.int32, length.shape, 1) != j
    length = jnp.sum(jnp.where(here, length, 0.0), axis=1, keepdims=True)
    row = lax.broadcasted_iota(jnp.int32, alive_ref.shape, 0).astype(F32)
    alive_ref[...] = jnp.where(row < length, 1.0, 0.0)
    kept_gain_ref[...] = gain_ref[...]
    keys = memory_ref.shape[2]
    for n in range(memory_ref.shape[0]):
        out_ref[n, :keys] = memory_ref[n, j].astype(BF16)
        bias = jnp.broadcast_to(bias_ref[n : n + 1, :], (BLOCK_LEN, keys))
        for at, value in ((keys, decay_ref[n, j]), (keys + BLOCK_LEN, bias)):
            for spot, term in enumerate(three_terms(value)):
                out_ref[n, at : at + BLOCK_LEN, spot * keys : (spot + 1) * keys] = term.astype(BF16)


def project_body(n, first, x_ref, x_next_ref, mine_ref, theirs_ref, out_ref, here_ref=None):
    k = lax.axis_index("k")
    tall, _, frames, features = x_ref.shape
    wide = out_ref.shape[0] // 2
    tiles = out_ref.shape[1] // BLOCK_LEN
    columns = tiles * LANES
    ones = jnp.ones((8, features), BF16)
    total, power = 0.0, 0.0
    for half, w_ref in ((k, mine_ref), (1 - k, theirs_ref)):
        x = x_next_ref[...] if first and half is not k else x_ref[:, half]
        x = x.reshape(tall * frames, features)
        total = total + dot(x, w_ref[:, n * columns : (n + 1) * columns])
        square = x.astype(F32) * x.astype(F32)
        high = square.astype(BF16)
        low = (square - high.astype(F32)).astype(BF16)
        power = power + dot(ones, high, EACH_ROW) + dot(ones, low, EACH_ROW)
    if here_ref is not None:
        here_ref[...] = x_ref[head_index(), 1 - k]
    total = total.astype(BF16)
    high, middle, low = three_terms(power)
    row = lax.broadcasted_iota(jnp.int32, power.shape, 0)
    terms = jnp.where(row == 0, high, jnp.where(row == 1, middle, jnp.where(row == 2, low, 0.0)))
    terms = terms.astype(BF16)
    for spot in range(2 * wide):
        j, c = divmod(spot, wide)
        start = c * frames + j * BLOCK_LEN
        for tile in range(tiles):
            out_ref[spot, tile * BLOCK_LEN : (tile + 1) * BLOCK_LEN, :] = total[
                start : start + BLOCK_LEN, tile * LANES : (tile + 1) * LANES
            ]
        lane = start // LANES * LANES
        out_ref[spot, tiles * BLOCK_LEN :, :] = terms[:, lane : lane + LANES]


def chips_sum_body(got_ref, out_ref):
    for half in range(2):
        value = got_ref[half, 0].astype(F32)
        for spot in range(1, got_ref.shape[1]):
            value = value + got_ref[half, spot].astype(F32)
        out_ref[half] = value


def recur_body(
    n,
    got_ref,
    memory_ref,
    packet_ref,
    decay_ref,
    bias_ref,
    alive_ref,
    gain_ref,
    out_ref,
    mine_ref,
    note_ref,
):
    b, c = lax.axis_index("b"), lax.axis_index("c")
    wide = out_ref.shape[0] // 2
    frames = 2 * BLOCK_LEN
    summed = [got_ref[half] for half in range(2)]
    tiles = got_ref.shape[1] // BLOCK_LEN
    power = jnp.sum(summed[0][tiles * BLOCK_LEN :], axis=0, keepdims=True)
    row = lax.broadcasted_iota(jnp.int32, (BLOCK_LEN, LANES), 0)
    lane = lax.broadcasted_iota(jnp.int32, (BLOCK_LEN, LANES), 1)
    first = lax.rem(c * frames, LANES) + b * BLOCK_LEN
    power = jnp.sum(jnp.where(lane == row + first, power, 0.0), axis=1, keepdims=True)
    scale = lax.rsqrt(power / D + EPS)

    def tile(half, spot):
        return summed[half][spot * BLOCK_LEN : (spot + 1) * BLOCK_LEN] * scale

    def unpacked(at):
        block = packet_ref[n, at : at + BLOCK_LEN, : 3 * LANES].astype(F32)
        return block[:, :LANES] + block[:, LANES : 2 * LANES] + block[:, 2 * LANES :]

    own_keys = memory_ref.shape[2]
    alive = alive_ref[...]
    extra = (decay_ref[n, b], unpacked(own_keys))
    bias = (jnp.broadcast_to(bias_ref[n : n + 1, :], extra[0].shape), unpacked(own_keys + BLOCK_LEN))
    queries, keys, totals = [], [], []
    for half in range(2):
        queries.append(tile(half, 0) * KEY_DIM ** (-0.5))
        keys.append(tile(half, 1) * alive)
        forget = tile(half, 2) + jnp.where(b == half, *bias)
        log_gate = jnp.minimum(forget, 0.0) - jnp.log1p(jnp.exp(-jnp.abs(forget)))
        total = (log_gate / TIME_CONSTANT + jnp.where(b == half, *extra)) * alive
        step = 1
        while step < BLOCK_LEN:
            total = total + jnp.where(row >= step, pltpu.roll(total, step, 0), 0.0)
            step *= 2
        totals.append(total)
    value_tiles = [tile(half, spot) for half in range(2) for spot in (3, 4)]
    values = jnp.concatenate(value_tiles, 1)
    gate = jnp.concatenate([tile(half, spot) for half in range(2) for spot in (5, 6)], 1)

    carried = [queries[half] * jnp.exp(totals[half]) for half in range(2)]
    read = dot(jnp.where(b == 0, carried[0], carried[1]).astype(BF16), memory_ref[n, b].astype(BF16))
    read = read + dot(jnp.where(b == 0, carried[1], carried[0]).astype(BF16), packet_ref[n, :own_keys])
    for spot in range(BLOCK_LEN):
        score = 0.0
        for half in range(2):
            spread = totals[half] - totals[half][spot : spot + 1]
            decay = jnp.exp(jnp.where(row >= spot, spread, 0.0))
            score = score + queries[half] * decay * keys[half][spot : spot + 1]
        score = jnp.sum(jnp.where(row >= spot, score, 0.0), axis=1, keepdims=True)
        read = read + score * values[spot : spot + 1]

    mean = jnp.mean(read * read, axis=1, keepdims=True)
    normed = read * lax.rsqrt(mean + EPS) * gain_ref[n : n + 1, :]
    gated = normed * (gate / (1.0 + jnp.exp(-gate))) * alive[:, :1]
    gated = gated.astype(BF16)
    width = out_ref.shape[2]
    for spot in range(2 * wide):
        half = spot // wide
        out_ref[spot] = gated[:, half * width : (half + 1) * width]

    weighted, kept = [], []
    for half in range(2):
        last = totals[half][BLOCK_LEN - 1 :]
        weighted.append(keys[half] * jnp.exp(last - totals[half]))
        block = jnp.zeros((BLOCK_LEN, LANES), F32)
        for spot, term in enumerate(three_terms(jnp.exp(last))):
            block = jnp.where(row == spot, term, block)
        kept.append(block)
    for ref, test in ((mine_ref, b == 0), (note_ref, b != 0)):
        parts = [jnp.where(test, *weighted), *value_tiles, jnp.where(test, *kept)]
        for spot, part in enumerate(parts):
            ref[spot * BLOCK_LEN : (spot + 1) * BLOCK_LEN] = part.astype(BF16)


def output_body(at, left_refs, right_refs, out_ref):
    k = lax.axis_index("k")
    wide = out_ref.shape[0] // 2
    for half, left_ref, right_ref in ((k, left_refs[0], right_refs[0]), (1 - k, left_refs[1], right_refs[1])):
        width = out_ref.shape[2]
        left = left_ref[...].reshape(2 * wide * BLOCK_LEN, left_ref.shape[2])
        partial = dot(left, right_ref[:, at : at + width]).astype(BF16)
        for spot in range(2 * wide):
            j, c = divmod(spot, wide)
            out_ref[2 * c + half, j * BLOCK_LEN : (j + 1) * BLOCK_LEN, :] = partial[
                spot * BLOCK_LEN : (spot + 1) * BLOCK_LEN
            ]


def output_same_frames_body(at, left_ref, mine_ref, theirs_ref, out_ref):
    output_body(at, (left_ref, left_ref), (mine_ref, theirs_ref), out_ref)


def output_same_features_body(left_ref, left_next_ref, right_ref, out_ref):
    output_body(0, (left_ref, left_next_ref), (right_ref, right_ref), out_ref)


def add_up(ref):
    value = ref[0].astype(F32)
    for spot in range(1, ref.shape[0]):
        value = value + ref[spot].astype(F32)
    return value.astype(BF16).astype(F32)


def quad_sum_body(got_ref, out_ref):
    write_copies(out_ref, add_up(got_ref).astype(BF16))


def next_stream_body(got_ref, x_ref, x_next_ref, out_ref):
    b, k = lax.axis_index("b"), lax.axis_index("k")
    frames = x_ref.shape[2]
    blocks = got_ref.shape[1] // frames
    first = (2 * lax.axis_index("near") + b) * (blocks // 2)
    summed = add_up(got_ref)
    for block in range(blocks):
        c, half = first + block // 2, block % 2
        residual = jnp.where(k == half, x_ref[c, k].astype(F32), x_next_ref[c].astype(F32))
        rows = slice(block * frames, (block + 1) * frames)
        value = (residual + summed[rows]).astype(BF16)
        for spot in range(out_ref.shape[0]):
            out_ref[spot, rows, :] = value


def last_stream_body(got_ref, x_ref, next_ref, out_ref):
    a, b, k = head_index(), lax.axis_index("b"), lax.axis_index("k")
    residual = jnp.where(b == k, x_ref[a, k].astype(F32), next_ref[...].astype(F32))
    out_ref[...] = (residual + add_up(got_ref)).astype(BF16)


def memory_body(memory_ref, mine_refs, theirs_ref, out_ref):
    b = lax.axis_index("b")
    keys = memory_ref.shape[2]
    row = lax.broadcasted_iota(jnp.int32, (keys, LANES), 0)
    lane = lax.broadcasted_iota(jnp.int32, (keys, LANES), 1)
    for n in range(memory_ref.shape[0]):
        for j, note in ((b, mine_refs[n][...]), (1 - b, theirs_ref[n])):
            parts = [note[at : at + BLOCK_LEN] for at in range(0, note.shape[0], BLOCK_LEN)]
            kept = jnp.sum(parts[-1].astype(F32), axis=0, keepdims=True)
            kept = jnp.sum(jnp.where(row == lane, kept, 0.0), axis=1, keepdims=True)
            values = jnp.concatenate(parts[1:-1], 1)
            out_ref[n, j] = kept * memory_ref[n, j] + dot(parts[0], values, EACH_COLUMN)


def memory_two_body(memory_ref, mine_ref, mine_next_ref, theirs_ref, out_ref):
    memory_body(memory_ref, (mine_ref, mine_next_ref), theirs_ref, out_ref)


def local(
    stream,
    lengths,
    input_norm_gain,
    query_projection,
    key_projection,
    forget_gate_weight,
    value_projection,
    output_gate_weight,
    forget_gate_bias,
    extra_frame_decay,
    head_norm_gain,
    output_projection,
    memory,
):
    quads, quad = lax.axis_size("far"), lax.axis_size(QUAD)
    tall, wide = lax.axis_size(HEAD), lax.axis_size("c")
    k = lax.axis_index("k")
    frames, features = stream.shape
    keys = query_projection.shape[2]
    values = value_projection.shape[2]
    layers = memory.shape[0]
    columns = 3 * keys + 2 * values
    decay = extra_frame_decay.reshape(layers, 2, BLOCK_LEN, keys)

    sent = kernel(copies_body, ((2 * tall, frames, features), BF16), stream)
    x = exchange(sent, ALONG_TP).reshape(tall, 2, frames, features)
    packet, alive, kept_gain = kernel(
        pack_state_body,
        [
            ((layers, keys + 2 * BLOCK_LEN, VALUE_DIM), BF16),
            ((BLOCK_LEN, LANES), F32),
            (head_norm_gain.shape, F32),
        ],
        memory,
        decay,
        forget_gate_bias,
        lengths[None],
        head_norm_gain,
    )
    weights = [
        query_projection,
        key_projection,
        forget_gate_weight,
        value_projection,
        output_gate_weight,
    ]
    weights = [
        (weight[n].astype(F32) * input_norm_gain[n][:, None]).astype(BF16)
        for n in range(layers)
        for weight in weights
    ]
    mine = jnp.concatenate([*weights, output_projection[0]], 1)
    theirs = other(mine, "k")
    packet = other(packet, "b")
    x, theirs = lax.optimization_barrier((x, theirs))
    x_next = other(lax.dynamic_index_in_dim(x, 1 - k, 1, keepdims=False), "k")

    mines, notes = [], []
    for n in range(layers):
        rows = columns // LANES * BLOCK_LEN + 8
        outs = [((2 * wide, rows, LANES), BF16), ((frames, features), BF16)]
        sent, *here = kernel(
            functools.partial(project_body, n, n == 0),
            outs if n + 1 == layers else outs[:1],
            x,
            x_next,
            mine,
            theirs,
        )
        got = exchange(sent, ALONG_X).reshape(2, wide, rows, LANES)
        got = kernel(chips_sum_body, ((2, rows, LANES), F32), got)
        note_shape = (6 * BLOCK_LEN, LANES)
        sent, own_note, note = kernel(
            functools.partial(recur_body, n),
            [((2 * wide, BLOCK_LEN, values), BF16), (note_shape, BF16), (note_shape, BF16)],
            got,
            memory,
            packet,
            decay,
            forget_gate_bias,
            alive,
            kept_gain,
        )
        mines.append(own_note)
        notes.append(note)
        got = exchange(sent, ALONG_X)
        if n + 1 < layers:
            sent = kernel(
                functools.partial(output_same_frames_body, layers * columns),
                ((2 * tall, frames, features), BF16),
                got,
                mine,
                theirs,
            )
            shape = (frames * 2 * tall // quad, features)
            got = exchange(sent.reshape(quad, *shape), QUAD)
            sent = kernel(quad_sum_body, ((quads, *shape), BF16), got)
            sent = kernel(next_stream_body, ((quad, *shape), BF16), exchange(sent, "far"), x, x_next)
            x = exchange(sent, QUAD).reshape(tall, 2, frames, features)
        else:
            theirs_got = other(jnp.concatenate([got, here[0].reshape(2, BLOCK_LEN, features)], 0), "k")
            sent = kernel(
                output_same_features_body,
                ((2 * tall, frames, features), BF16),
                got,
                theirs_got[: 2 * wide],
                output_projection[n],
            )
            notes, sent = lax.optimization_barrier((notes, sent))
            theirs_note = other(jnp.stack(notes), "b")
            current = kernel(
                last_stream_body,
                (stream.shape, BF16),
                exchange(sent, ALONG_TP),
                x,
                theirs_got[2 * wide :].reshape(frames, features),
            )
            fresh = kernel(memory_two_body, (memory.shape, F32), memory, *mines, theirs_note)
    return current, fresh


def solution(mesh):
    grp, tp, dp = (mesh.shape[name] for name in ("grp", "tp", "dp"))
    fine = Mesh(
        mesh.devices.reshape(grp, tp // 4, 2, 2, dp // 2, 2), ("grp", *ALONG_TP, "c", "k")
    )
    tp, dp = ALONG_TP, ("c", "k")
    group_tp, group_dp = ("grp", *tp), ("grp", *dp)
    placed = (
        P(group_tp, dp),
        P(group_dp),
        P(None, dp),
        P(None, dp, tp),
        P(None, dp, tp),
        P(None, dp, tp),
        P(None, dp, tp),
        P(None, dp, tp),
        P(None, tp),
        P(None, group_dp, tp),
        P(),
        P(None, tp, dp),
        P(None, group_dp, tp, None),
    )

    return jax.shard_map(
        local,
        mesh=fine,
        in_specs=placed,
        out_specs=(P(group_tp, dp), P(None, group_dp, tp, None)),
        check_vma=False,
    )
```

```python
import functools

import jax
import jax.numpy as jnp
from jax import lax
from jax.experimental import pallas as pl
from jax.experimental.pallas import tpu as pltpu
from jax.sharding import Mesh
from jax.sharding import PartitionSpec as P


D = 4096
KEY_DIM = 256
VALUE_DIM = 512
BLOCK_LEN = 16

EPS = 1e-06
TIME_CONSTANT = 16.0

ALONG_TP = ("far", "near", "b")
QUAD = ("near", "b")
HEAD = ("far", "near")
ALONG_X = ("b", "c")


def exchange(array, axes):
    return lax.all_to_all(array, axes, 0, 0, tiled=True)


def other(array, axis):
    return lax.ppermute(array, axis, [(0, 1), (1, 0)])


LANES = 128
VMEM_LIMIT = 8 * 2**20
F32, BF16 = jnp.float32, jnp.bfloat16
EACH_ROW = (((1,), (1,)), ((), ()))
EACH_COLUMN = (((0,), (0,)), ((), ()))


def dot(left, right, dims=(((1,), (0,)), ((), ()))):
    return lax.dot_general(left, right, dims, preferred_element_type=F32)


def kernel(body, outs, *args):
    vmem = pl.BlockSpec(memory_space=pltpu.VMEM)
    several = isinstance(outs, list)
    shapes = [jax.ShapeDtypeStruct(*out) for out in (outs if several else [outs])]
    return pl.pallas_call(
        body,
        out_shape=shapes if several else shapes[0],
        in_specs=[vmem] * len(args),
        out_specs=[vmem] * len(shapes) if several else vmem,
        compiler_params=pltpu.CompilerParams(vmem_limit_bytes=VMEM_LIMIT),
    )(*args)


def three_terms(value):
    high = value.astype(BF16).astype(F32)
    middle = (value - high).astype(BF16).astype(F32)
    return high, middle, value - high - middle


def head_index():
    return lax.axis_index("far") * lax.axis_size("near") + lax.axis_index("near")


def write_copies(out_ref, value):
    for spot in range(out_ref.shape[0]):
        out_ref[spot] = value


def copies_body(in_ref, out_ref):
    write_copies(out_ref, in_ref[...])


def pack_state_body(memory_ref, decay_ref, bias_ref, lengths_ref, gain_ref, out_ref, alive_ref, kept_gain_ref):
    j = 1 - lax.axis_index("b")
    length = lengths_ref[...].astype(F32)
    here = lax.broadcasted_iota(jnp.int32, length.shape, 1) != j
    length = jnp.sum(jnp.where(here, length, 0.0), axis=1, keepdims=True)
    row = lax.broadcasted_iota(jnp.int32, alive_ref.shape, 0).astype(F32)
    alive_ref[...] = jnp.where(row < length, 1.0, 0.0)
    kept_gain_ref[...] = gain_ref[...]
    keys = memory_ref.shape[2]
    for n in range(memory_ref.shape[0]):
        out_ref[n, :keys] = memory_ref[n, j].astype(BF16)
        bias = jnp.broadcast_to(bias_ref[n : n + 1, :], (BLOCK_LEN, keys))
        for at, value in ((keys, decay_ref[n, j]), (keys + BLOCK_LEN, bias)):
            for spot, term in enumerate(three_terms(value)):
                out_ref[n, at : at + BLOCK_LEN, spot * keys : (spot + 1) * keys] = term.astype(BF16)


def project_body(n, first, x_ref, x_next_ref, mine_ref, theirs_ref, out_ref, here_ref=None):
    k = lax.axis_index("k")
    tall, _, frames, features = x_ref.shape
    wide = out_ref.shape[0] // 2
    tiles = out_ref.shape[1] // BLOCK_LEN
    columns = tiles * LANES
    ones = jnp.ones((8, features), BF16)
    total, power = 0.0, 0.0
    for half, w_ref in ((k, mine_ref), (1 - k, theirs_ref)):
        x = x_next_ref[...] if first and half is not k else x_ref[:, half]
        x = x.reshape(tall * frames, features)
        total = total + dot(x, w_ref[:, n * columns : (n + 1) * columns])
        square = x.astype(F32) * x.astype(F32)
        high = square.astype(BF16)
        low = (square - high.astype(F32)).astype(BF16)
        power = power + dot(ones, high, EACH_ROW) + dot(ones, low, EACH_ROW)
    if here_ref is not None:
        here_ref[...] = x_ref[head_index(), 1 - k]
    total = total.astype(BF16)
    high, middle, low = three_terms(power)
    row = lax.broadcasted_iota(jnp.int32, power.shape, 0)
    terms = jnp.where(row == 0, high, jnp.where(row == 1, middle, jnp.where(row == 2, low, 0.0)))
    terms = terms.astype(BF16)
    for spot in range(2 * wide):
        j, c = divmod(spot, wide)
        start = c * frames + j * BLOCK_LEN
        for tile in range(tiles):
            out_ref[spot, tile * BLOCK_LEN : (tile + 1) * BLOCK_LEN, :] = total[
                start : start + BLOCK_LEN, tile * LANES : (tile + 1) * LANES
            ]
        lane = start // LANES * LANES
        out_ref[spot, tiles * BLOCK_LEN :, :] = terms[:, lane : lane + LANES]


def chips_sum_body(got_ref, out_ref):
    for half in range(2):
        value = got_ref[half, 0].astype(F32)
        for spot in range(1, got_ref.shape[1]):
            value = value + got_ref[half, spot].astype(F32)
        out_ref[half] = value


def recur_body(
    n,
    got_ref,
    memory_ref,
    packet_ref,
    decay_ref,
    bias_ref,
    alive_ref,
    gain_ref,
    out_ref,
    mine_ref,
    note_ref,
):
    b, c = lax.axis_index("b"), lax.axis_index("c")
    wide = out_ref.shape[0] // 2
    frames = 2 * BLOCK_LEN
    summed = [got_ref[half] for half in range(2)]
    tiles = got_ref.shape[1] // BLOCK_LEN
    power = jnp.sum(summed[0][tiles * BLOCK_LEN :], axis=0, keepdims=True)
    row = lax.broadcasted_iota(jnp.int32, (BLOCK_LEN, LANES), 0)
    lane = lax.broadcasted_iota(jnp.int32, (BLOCK_LEN, LANES), 1)
    first = lax.rem(c * frames, LANES) + b * BLOCK_LEN
    power = jnp.sum(jnp.where(lane == row + first, power, 0.0), axis=1, keepdims=True)
    scale = lax.rsqrt(power / D + EPS)

    def tile(half, spot):
        return summed[half][spot * BLOCK_LEN : (spot + 1) * BLOCK_LEN] * scale

    def unpacked(at):
        block = packet_ref[n, at : at + BLOCK_LEN, : 3 * LANES].astype(F32)
        return block[:, :LANES] + block[:, LANES : 2 * LANES] + block[:, 2 * LANES :]

    own_keys = memory_ref.shape[2]
    alive = alive_ref[...]
    extra = (decay_ref[n, b], unpacked(own_keys))
    bias = (jnp.broadcast_to(bias_ref[n : n + 1, :], extra[0].shape), unpacked(own_keys + BLOCK_LEN))
    queries, keys, totals = [], [], []
    for half in range(2):
        queries.append(tile(half, 0) * KEY_DIM ** (-0.5))
        keys.append(tile(half, 1) * alive)
        forget = tile(half, 2) + jnp.where(b == half, *bias)
        log_gate = jnp.minimum(forget, 0.0) - jnp.log1p(jnp.exp(-jnp.abs(forget)))
        total = (log_gate / TIME_CONSTANT + jnp.where(b == half, *extra)) * alive
        step = 1
        while step < BLOCK_LEN:
            total = total + jnp.where(row >= step, pltpu.roll(total, step, 0), 0.0)
            step *= 2
        totals.append(total)
    value_tiles = [tile(half, spot) for half in range(2) for spot in (3, 4)]
    values = jnp.concatenate(value_tiles, 1)
    gate = jnp.concatenate([tile(half, spot) for half in range(2) for spot in (5, 6)], 1)

    carried = [queries[half] * jnp.exp(totals[half]) for half in range(2)]
    read = dot(jnp.where(b == 0, carried[0], carried[1]).astype(BF16), memory_ref[n, b].astype(BF16))
    read = read + dot(jnp.where(b == 0, carried[1], carried[0]).astype(BF16), packet_ref[n, :own_keys])
    for spot in range(BLOCK_LEN):
        score = 0.0
        for half in range(2):
            spread = totals[half] - totals[half][spot : spot + 1]
            decay = jnp.exp(jnp.where(row >= spot, spread, 0.0))
            score = score + queries[half] * decay * keys[half][spot : spot + 1]
        score = jnp.sum(jnp.where(row >= spot, score, 0.0), axis=1, keepdims=True)
        read = read + score * values[spot : spot + 1]

    mean = jnp.mean(read * read, axis=1, keepdims=True)
    normed = read * lax.rsqrt(mean + EPS) * gain_ref[n : n + 1, :]
    gated = normed * (gate / (1.0 + jnp.exp(-gate))) * alive[:, :1]
    gated = gated.astype(BF16)
    width = out_ref.shape[2]
    for spot in range(2 * wide):
        half = spot // wide
        out_ref[spot] = gated[:, half * width : (half + 1) * width]

    weighted, kept = [], []
    for half in range(2):
        last = totals[half][BLOCK_LEN - 1 :]
        weighted.append(keys[half] * jnp.exp(last - totals[half]))
        block = jnp.zeros((BLOCK_LEN, LANES), F32)
        for spot, term in enumerate(three_terms(jnp.exp(last))):
            block = jnp.where(row == spot, term, block)
        kept.append(block)
    for ref, test in ((mine_ref, b == 0), (note_ref, b != 0)):
        parts = [jnp.where(test, *weighted), *value_tiles, jnp.where(test, *kept)]
        for spot, part in enumerate(parts):
            ref[spot * BLOCK_LEN : (spot + 1) * BLOCK_LEN] = part.astype(BF16)


def output_body(at, left_refs, right_refs, out_ref):
    k = lax.axis_index("k")
    wide = out_ref.shape[0] // 2
    for half, left_ref, right_ref in ((k, left_refs[0], right_refs[0]), (1 - k, left_refs[1], right_refs[1])):
        width = out_ref.shape[2]
        left = left_ref[...].reshape(2 * wide * BLOCK_LEN, left_ref.shape[2])
        partial = dot(left, right_ref[:, at : at + width]).astype(BF16)
        for spot in range(2 * wide):
            j, c = divmod(spot, wide)
            out_ref[2 * c + half, j * BLOCK_LEN : (j + 1) * BLOCK_LEN, :] = partial[
                spot * BLOCK_LEN : (spot + 1) * BLOCK_LEN
            ]


def output_same_frames_body(at, left_ref, mine_ref, theirs_ref, out_ref):
    output_body(at, (left_ref, left_ref), (mine_ref, theirs_ref), out_ref)


def output_same_features_body(left_ref, left_next_ref, right_ref, out_ref):
    output_body(0, (left_ref, left_next_ref), (right_ref, right_ref), out_ref)


def add_up(ref):
    value = ref[0].astype(F32)
    for spot in range(1, ref.shape[0]):
        value = value + ref[spot].astype(F32)
    return value.astype(BF16).astype(F32)


def quad_sum_body(got_ref, out_ref):
    out_ref[...] = add_up(got_ref).astype(BF16)


def next_stream_body(got_ref, x_ref, x_next_ref, out_ref):
    b, k = lax.axis_index("b"), lax.axis_index("k")
    frames = x_ref.shape[2]
    blocks = got_ref.shape[1] // frames
    first = (2 * lax.axis_index("near") + b) * (blocks // 2)
    summed = add_up(got_ref)
    for block in range(blocks):
        c, half = first + block // 2, block % 2
        residual = jnp.where(k == half, x_ref[c, k].astype(F32), x_next_ref[c].astype(F32))
        rows = slice(block * frames, (block + 1) * frames)
        value = (residual + summed[rows]).astype(BF16)
        for spot in range(out_ref.shape[0]):
            out_ref[spot, rows, :] = value


def last_stream_body(got_ref, x_ref, next_ref, out_ref):
    a, b, k = head_index(), lax.axis_index("b"), lax.axis_index("k")
    residual = jnp.where(b == k, x_ref[a, k].astype(F32), next_ref[...].astype(F32))
    out_ref[...] = (residual + add_up(got_ref)).astype(BF16)


def memory_body(memory_ref, mine_refs, theirs_ref, out_ref):
    b = lax.axis_index("b")
    keys = memory_ref.shape[2]
    row = lax.broadcasted_iota(jnp.int32, (keys, LANES), 0)
    lane = lax.broadcasted_iota(jnp.int32, (keys, LANES), 1)
    for n in range(memory_ref.shape[0]):
        for j, note in ((b, mine_refs[n][...]), (1 - b, theirs_ref[n])):
            parts = [note[at : at + BLOCK_LEN] for at in range(0, note.shape[0], BLOCK_LEN)]
            kept = jnp.sum(parts[-1].astype(F32), axis=0, keepdims=True)
            kept = jnp.sum(jnp.where(row == lane, kept, 0.0), axis=1, keepdims=True)
            values = jnp.concatenate(parts[1:-1], 1)
            out_ref[n, j] = kept * memory_ref[n, j] + dot(parts[0], values, EACH_COLUMN)


def memory_two_body(memory_ref, mine_ref, mine_next_ref, theirs_ref, out_ref):
    memory_body(memory_ref, (mine_ref, mine_next_ref), theirs_ref, out_ref)


def local(
    stream,
    lengths,
    input_norm_gain,
    query_projection,
    key_projection,
    forget_gate_weight,
    value_projection,
    output_gate_weight,
    forget_gate_bias,
    extra_frame_decay,
    head_norm_gain,
    output_projection,
    memory,
):
    quad = lax.axis_size(QUAD)
    tall, wide = lax.axis_size(HEAD), lax.axis_size("c")
    k = lax.axis_index("k")
    frames, features = stream.shape
    keys = query_projection.shape[2]
    values = value_projection.shape[2]
    layers = memory.shape[0]
    columns = 3 * keys + 2 * values
    decay = extra_frame_decay.reshape(layers, 2, BLOCK_LEN, keys)

    sent = kernel(copies_body, ((2 * tall, frames, features), BF16), stream)
    x = exchange(sent, ALONG_TP).reshape(tall, 2, frames, features)
    packet, alive, kept_gain = kernel(
        pack_state_body,
        [
            ((layers, keys + 2 * BLOCK_LEN, VALUE_DIM), BF16),
            ((BLOCK_LEN, LANES), F32),
            (head_norm_gain.shape, F32),
        ],
        memory,
        decay,
        forget_gate_bias,
        lengths[None],
        head_norm_gain,
    )
    weights = [
        query_projection,
        key_projection,
        forget_gate_weight,
        value_projection,
        output_gate_weight,
    ]
    weights = [
        (weight[n].astype(F32) * input_norm_gain[n][:, None]).astype(BF16)
        for n in range(layers)
        for weight in weights
    ]
    mine = jnp.concatenate([*weights, output_projection[0]], 1)
    theirs = other(mine, "k")
    packet = other(packet, "b")
    x, theirs = lax.optimization_barrier((x, theirs))
    x_next = other(lax.dynamic_index_in_dim(x, 1 - k, 1, keepdims=False), "k")

    mines, notes = [], []
    for n in range(layers):
        rows = columns // LANES * BLOCK_LEN + 8
        outs = [((2 * wide, rows, LANES), BF16), ((frames, features), BF16)]
        sent, *here = kernel(
            functools.partial(project_body, n, n == 0),
            outs if n + 1 == layers else outs[:1],
            x,
            x_next,
            mine,
            theirs,
        )
        got = exchange(sent, ALONG_X).reshape(2, wide, rows, LANES)
        got = kernel(chips_sum_body, ((2, rows, LANES), F32), got)
        note_shape = (6 * BLOCK_LEN, LANES)
        sent, own_note, note = kernel(
            functools.partial(recur_body, n),
            [((2 * wide, BLOCK_LEN, values), BF16), (note_shape, BF16), (note_shape, BF16)],
            got,
            memory,
            packet,
            decay,
            forget_gate_bias,
            alive,
            kept_gain,
        )
        mines.append(own_note)
        notes.append(note)
        got = exchange(sent, ALONG_X)
        if n + 1 < layers:
            sent = kernel(
                functools.partial(output_same_frames_body, layers * columns),
                ((2 * tall, frames, features), BF16),
                got,
                mine,
                theirs,
            )
            shape = (frames * 2 * tall // quad, features)
            got = exchange(sent.reshape(quad, *shape), QUAD)
            got = lax.all_gather(kernel(quad_sum_body, (shape, BF16), got), "far")
            sent = kernel(next_stream_body, ((quad, *shape), BF16), got, x, x_next)
            x = exchange(sent, QUAD).reshape(tall, 2, frames, features)
        else:
            theirs_got = other(jnp.concatenate([got, here[0].reshape(2, BLOCK_LEN, features)], 0), "k")
            sent = kernel(
                output_same_features_body,
                ((2 * tall, frames, features), BF16),
                got,
                theirs_got[: 2 * wide],
                output_projection[n],
            )
            notes, sent = lax.optimization_barrier((notes, sent))
            theirs_note = other(jnp.stack(notes), "b")
            current = kernel(
                last_stream_body,
                (stream.shape, BF16),
                exchange(sent, ALONG_TP),
                x,
                theirs_got[2 * wide :].reshape(frames, features),
            )
            fresh = kernel(memory_two_body, (memory.shape, F32), memory, *mines, theirs_note)
    return current, fresh


def solution(mesh):
    grp, tp, dp = (mesh.shape[name] for name in ("grp", "tp", "dp"))
    fine = Mesh(
        mesh.devices.reshape(grp, tp // 4, 2, 2, dp // 2, 2), ("grp", *ALONG_TP, "c", "k")
    )
    tp, dp = ALONG_TP, ("c", "k")
    group_tp, group_dp = ("grp", *tp), ("grp", *dp)
    placed = (
        P(group_tp, dp),
        P(group_dp),
        P(None, dp),
        P(None, dp, tp),
        P(None, dp, tp),
        P(None, dp, tp),
        P(None, dp, tp),
        P(None, dp, tp),
        P(None, tp),
        P(None, group_dp, tp),
        P(),
        P(None, tp, dp),
        P(None, group_dp, tp, None),
    )

    return jax.shard_map(
        local,
        mesh=fine,
        in_specs=placed,
        out_specs=(P(group_tp, dp), P(None, group_dp, tp, None)),
        check_vma=False,
    )
```

```python
import functools

import jax
import jax.numpy as jnp
from jax import lax
from jax.experimental import pallas as pl
from jax.experimental.pallas import tpu as pltpu
from jax.sharding import Mesh
from jax.sharding import PartitionSpec as P


D = 4096
KEY_DIM = 256
VALUE_DIM = 512
BLOCK_LEN = 16

EPS = 1e-06
TIME_CONSTANT = 16.0

ALONG_TP = ("far", "near", "b")
QUAD = ("near", "b")
HEAD = ("far", "near")
ALONG_X = ("b", "c")


def exchange(array, axes):
    return lax.all_to_all(array, axes, 0, 0, tiled=True)


def other(array, axis):
    return lax.ppermute(array, axis, [(0, 1), (1, 0)])


LANES = 128
VMEM_LIMIT = 8 * 2**20
F32, BF16 = jnp.float32, jnp.bfloat16
EACH_ROW = (((1,), (1,)), ((), ()))
EACH_COLUMN = (((0,), (0,)), ((), ()))


def dot(left, right, dims=(((1,), (0,)), ((), ()))):
    return lax.dot_general(left, right, dims, preferred_element_type=F32)


def kernel(body, outs, *args):
    vmem = pl.BlockSpec(memory_space=pltpu.VMEM)
    several = isinstance(outs, list)
    shapes = [jax.ShapeDtypeStruct(*out) for out in (outs if several else [outs])]
    return pl.pallas_call(
        body,
        out_shape=shapes if several else shapes[0],
        in_specs=[vmem] * len(args),
        out_specs=[vmem] * len(shapes) if several else vmem,
        compiler_params=pltpu.CompilerParams(vmem_limit_bytes=VMEM_LIMIT),
    )(*args)


def three_terms(value):
    high = value.astype(BF16).astype(F32)
    middle = (value - high).astype(BF16).astype(F32)
    return high, middle, value - high - middle


def head_index():
    return lax.axis_index("far") * lax.axis_size("near") + lax.axis_index("near")


def write_copies(out_ref, value):
    for spot in range(out_ref.shape[0]):
        out_ref[spot] = value


def copies_body(in_ref, out_ref):
    write_copies(out_ref, in_ref[...])


def pack_state_body(memory_ref, decay_ref, bias_ref, lengths_ref, gain_ref, out_ref, alive_ref, kept_gain_ref):
    j = 1 - lax.axis_index("b")
    length = lengths_ref[...].astype(F32)
    here = lax.broadcasted_iota(jnp.int32, length.shape, 1) != j
    length = jnp.sum(jnp.where(here, length, 0.0), axis=1, keepdims=True)
    row = lax.broadcasted_iota(jnp.int32, alive_ref.shape, 0).astype(F32)
    alive_ref[...] = jnp.where(row < length, 1.0, 0.0)
    kept_gain_ref[...] = gain_ref[...]
    keys = memory_ref.shape[2]
    for n in range(memory_ref.shape[0]):
        out_ref[n, :keys] = memory_ref[n, j].astype(BF16)
        bias = jnp.broadcast_to(bias_ref[n : n + 1, :], (BLOCK_LEN, keys))
        for at, value in ((keys, decay_ref[n, j]), (keys + BLOCK_LEN, bias)):
            for spot, term in enumerate(three_terms(value)):
                out_ref[n, at : at + BLOCK_LEN, spot * keys : (spot + 1) * keys] = term.astype(BF16)


def project_body(n, first, x_ref, x_next_ref, mine_ref, theirs_ref, out_ref, here_ref=None):
    k = lax.axis_index("k")
    tall, _, frames, features = x_ref.shape
    wide = out_ref.shape[0] // 2
    tiles = out_ref.shape[1] // BLOCK_LEN
    columns = tiles * LANES
    ones = jnp.ones((8, features), BF16)
    total, power = 0.0, 0.0
    for half, w_ref in ((k, mine_ref), (1 - k, theirs_ref)):
        x = x_next_ref[...] if first and half is not k else x_ref[:, half]
        x = x.reshape(tall * frames, features)
        total = total + dot(x, w_ref[:, n * columns : (n + 1) * columns])
        square = x.astype(F32) * x.astype(F32)
        high = square.astype(BF16)
        low = (square - high.astype(F32)).astype(BF16)
        power = power + dot(ones, high, EACH_ROW) + dot(ones, low, EACH_ROW)
    if here_ref is not None:
        here_ref[...] = x_ref[head_index(), 1 - k]
    total = total.astype(BF16)
    high, middle, low = three_terms(power)
    row = lax.broadcasted_iota(jnp.int32, power.shape, 0)
    terms = jnp.where(row == 0, high, jnp.where(row == 1, middle, jnp.where(row == 2, low, 0.0)))
    terms = terms.astype(BF16)
    for spot in range(2 * wide):
        j, c = divmod(spot, wide)
        start = c * frames + j * BLOCK_LEN
        for tile in range(tiles):
            out_ref[spot, tile * BLOCK_LEN : (tile + 1) * BLOCK_LEN, :] = total[
                start : start + BLOCK_LEN, tile * LANES : (tile + 1) * LANES
            ]
        lane = start // LANES * LANES
        out_ref[spot, tiles * BLOCK_LEN :, :] = terms[:, lane : lane + LANES]


def chips_sum_body(got_ref, out_ref):
    for half in range(2):
        value = got_ref[half, 0].astype(F32)
        for spot in range(1, got_ref.shape[1]):
            value = value + got_ref[half, spot].astype(F32)
        out_ref[half] = value


def recur_body(
    n,
    got_ref,
    memory_ref,
    packet_ref,
    decay_ref,
    bias_ref,
    alive_ref,
    gain_ref,
    out_ref,
    mine_ref,
    note_ref,
):
    b, c = lax.axis_index("b"), lax.axis_index("c")
    wide = out_ref.shape[0] // 2
    frames = 2 * BLOCK_LEN
    summed = [got_ref[half] for half in range(2)]
    tiles = got_ref.shape[1] // BLOCK_LEN
    power = jnp.sum(summed[0][tiles * BLOCK_LEN :], axis=0, keepdims=True)
    row = lax.broadcasted_iota(jnp.int32, (BLOCK_LEN, LANES), 0)
    lane = lax.broadcasted_iota(jnp.int32, (BLOCK_LEN, LANES), 1)
    first = lax.rem(c * frames, LANES) + b * BLOCK_LEN
    power = jnp.sum(jnp.where(lane == row + first, power, 0.0), axis=1, keepdims=True)
    scale = lax.rsqrt(power / D + EPS)

    def tile(half, spot):
        return summed[half][spot * BLOCK_LEN : (spot + 1) * BLOCK_LEN] * scale

    def unpacked(at):
        block = packet_ref[n, at : at + BLOCK_LEN, : 3 * LANES].astype(F32)
        return block[:, :LANES] + block[:, LANES : 2 * LANES] + block[:, 2 * LANES :]

    own_keys = memory_ref.shape[2]
    alive = alive_ref[...]
    extra = (decay_ref[n, b], unpacked(own_keys))
    bias = (jnp.broadcast_to(bias_ref[n : n + 1, :], extra[0].shape), unpacked(own_keys + BLOCK_LEN))
    queries, keys, totals = [], [], []
    for half in range(2):
        queries.append(tile(half, 0) * KEY_DIM ** (-0.5))
        keys.append(tile(half, 1) * alive)
        forget = tile(half, 2) + jnp.where(b == half, *bias)
        log_gate = jnp.minimum(forget, 0.0) - jnp.log1p(jnp.exp(-jnp.abs(forget)))
        total = (log_gate / TIME_CONSTANT + jnp.where(b == half, *extra)) * alive
        step = 1
        while step < BLOCK_LEN:
            total = total + jnp.where(row >= step, pltpu.roll(total, step, 0), 0.0)
            step *= 2
        totals.append(total)
    value_tiles = [tile(half, spot) for half in range(2) for spot in (3, 4)]
    values = jnp.concatenate(value_tiles, 1)
    gate = jnp.concatenate([tile(half, spot) for half in range(2) for spot in (5, 6)], 1)

    carried = [queries[half] * jnp.exp(totals[half]) for half in range(2)]
    read = dot(jnp.where(b == 0, carried[0], carried[1]).astype(BF16), memory_ref[n, b].astype(BF16))
    read = read + dot(jnp.where(b == 0, carried[1], carried[0]).astype(BF16), packet_ref[n, :own_keys])
    for spot in range(BLOCK_LEN):
        score = 0.0
        for half in range(2):
            spread = totals[half] - totals[half][spot : spot + 1]
            decay = jnp.exp(jnp.where(row >= spot, spread, 0.0))
            score = score + queries[half] * decay * keys[half][spot : spot + 1]
        score = jnp.sum(jnp.where(row >= spot, score, 0.0), axis=1, keepdims=True)
        read = read + score * values[spot : spot + 1]

    mean = jnp.mean(read * read, axis=1, keepdims=True)
    normed = read * lax.rsqrt(mean + EPS) * gain_ref[n : n + 1, :]
    gated = normed * (gate / (1.0 + jnp.exp(-gate))) * alive[:, :1]
    gated = gated.astype(BF16)
    width = out_ref.shape[2]
    for spot in range(2 * wide):
        half = spot // wide
        out_ref[spot] = gated[:, half * width : (half + 1) * width]

    weighted, kept = [], []
    for half in range(2):
        last = totals[half][BLOCK_LEN - 1 :]
        weighted.append(keys[half] * jnp.exp(last - totals[half]))
        block = jnp.zeros((BLOCK_LEN, LANES), F32)
        for spot, term in enumerate(three_terms(jnp.exp(last))):
            block = jnp.where(row == spot, term, block)
        kept.append(block)
    for ref, test in ((mine_ref, b == 0), (note_ref, b != 0)):
        parts = [jnp.where(test, *weighted), *value_tiles, jnp.where(test, *kept)]
        for spot, part in enumerate(parts):
            ref[spot * BLOCK_LEN : (spot + 1) * BLOCK_LEN] = part.astype(BF16)


def output_body(at, turns, left_refs, right_refs, out_ref):
    k = lax.axis_index("k")
    wide = out_ref.shape[0] // 2
    for half, left_ref, right_ref in ((k, left_refs[0], right_refs[0]), (1 - k, left_refs[1], right_refs[1])):
        width = out_ref.shape[2]
        left = left_ref[...].reshape(2 * wide * BLOCK_LEN, left_ref.shape[2])
        partial = dot(left, right_ref[:, at : at + width]).astype(BF16)
        for spot in range(2 * wide):
            j, c = divmod(spot, wide)
            place = 2 * c + half
            if turns is not None:
                place = (2 * (c % 2) + half) * turns + c // 2
            out_ref[place, j * BLOCK_LEN : (j + 1) * BLOCK_LEN, :] = partial[
                spot * BLOCK_LEN : (spot + 1) * BLOCK_LEN
            ]


def output_same_frames_body(at, left_ref, mine_ref, theirs_ref, out_ref):
    output_body(at, None, (left_ref, left_ref), (mine_ref, theirs_ref), out_ref)


def output_same_features_body(turns, left_ref, left_next_ref, right_ref, out_ref):
    output_body(0, turns, (left_ref, left_next_ref), (right_ref, right_ref), out_ref)


def add_up(ref):
    value = ref[0].astype(F32)
    for spot in range(1, ref.shape[0]):
        value = value + ref[spot].astype(F32)
    return value.astype(BF16).astype(F32)


def quad_sum_body(got_ref, out_ref):
    out_ref[...] = add_up(got_ref).astype(BF16)


def next_stream_body(got_ref, x_ref, x_next_ref, out_ref):
    b, k = lax.axis_index("b"), lax.axis_index("k")
    frames = x_ref.shape[2]
    blocks = got_ref.shape[1] // frames
    first = (2 * lax.axis_index("near") + b) * (blocks // 2)
    summed = add_up(got_ref)
    for block in range(blocks):
        c, half = first + block // 2, block % 2
        residual = jnp.where(k == half, x_ref[c, k].astype(F32), x_next_ref[c].astype(F32))
        rows = slice(block * frames, (block + 1) * frames)
        value = (residual + summed[rows]).astype(BF16)
        for spot in range(out_ref.shape[0]):
            out_ref[spot, rows, :] = value


def last_stream_body(got_ref, x_ref, next_ref, out_ref):
    a, b, k = head_index(), lax.axis_index("b"), lax.axis_index("k")
    residual = jnp.where(b == k, x_ref[a, k].astype(F32), next_ref[...].astype(F32))
    out_ref[...] = (residual + add_up(got_ref)).astype(BF16)


def memory_body(memory_ref, mine_refs, theirs_ref, out_ref):
    b = lax.axis_index("b")
    keys = memory_ref.shape[2]
    row = lax.broadcasted_iota(jnp.int32, (keys, LANES), 0)
    lane = lax.broadcasted_iota(jnp.int32, (keys, LANES), 1)
    for n in range(memory_ref.shape[0]):
        for j, note in ((b, mine_refs[n][...]), (1 - b, theirs_ref[n])):
            parts = [note[at : at + BLOCK_LEN] for at in range(0, note.shape[0], BLOCK_LEN)]
            kept = jnp.sum(parts[-1].astype(F32), axis=0, keepdims=True)
            kept = jnp.sum(jnp.where(row == lane, kept, 0.0), axis=1, keepdims=True)
            values = jnp.concatenate(parts[1:-1], 1)
            out_ref[n, j] = kept * memory_ref[n, j] + dot(parts[0], values, EACH_COLUMN)


def memory_two_body(memory_ref, mine_ref, mine_next_ref, theirs_ref, out_ref):
    memory_body(memory_ref, (mine_ref, mine_next_ref), theirs_ref, out_ref)


def local(
    stream,
    lengths,
    input_norm_gain,
    query_projection,
    key_projection,
    forget_gate_weight,
    value_projection,
    output_gate_weight,
    forget_gate_bias,
    extra_frame_decay,
    head_norm_gain,
    output_projection,
    memory,
):
    quad = lax.axis_size(QUAD)
    tall, wide = lax.axis_size(HEAD), lax.axis_size("c")
    k = lax.axis_index("k")
    frames, features = stream.shape
    keys = query_projection.shape[2]
    values = value_projection.shape[2]
    layers = memory.shape[0]
    columns = 3 * keys + 2 * values
    decay = extra_frame_decay.reshape(layers, 2, BLOCK_LEN, keys)

    sent = kernel(copies_body, ((2 * tall, frames, features), BF16), stream)
    x = exchange(sent, ALONG_TP).reshape(tall, 2, frames, features)
    packet, alive, kept_gain = kernel(
        pack_state_body,
        [
            ((layers, keys + 2 * BLOCK_LEN, VALUE_DIM), BF16),
            ((BLOCK_LEN, LANES), F32),
            (head_norm_gain.shape, F32),
        ],
        memory,
        decay,
        forget_gate_bias,
        lengths[None],
        head_norm_gain,
    )
    weights = [
        query_projection,
        key_projection,
        forget_gate_weight,
        value_projection,
        output_gate_weight,
    ]
    weights = [
        (weight[n].astype(F32) * input_norm_gain[n][:, None]).astype(BF16)
        for n in range(layers)
        for weight in weights
    ]
    mine = jnp.concatenate([*weights, output_projection[0]], 1)
    theirs = other(mine, "k")
    packet = other(packet, "b")
    x, theirs = lax.optimization_barrier((x, theirs))
    x_next = other(lax.dynamic_index_in_dim(x, 1 - k, 1, keepdims=False), "k")

    mines, notes = [], []
    for n in range(layers):
        rows = columns // LANES * BLOCK_LEN + 8
        outs = [((2 * wide, rows, LANES), BF16), ((frames, features), BF16)]
        sent, *here = kernel(
            functools.partial(project_body, n, n == 0),
            outs if n + 1 == layers else outs[:1],
            x,
            x_next,
            mine,
            theirs,
        )
        got = exchange(sent, ALONG_X).reshape(2, wide, rows, LANES)
        got = kernel(chips_sum_body, ((2, rows, LANES), F32), got)
        note_shape = (6 * BLOCK_LEN, LANES)
        sent, own_note, note = kernel(
            functools.partial(recur_body, n),
            [((2 * wide, BLOCK_LEN, values), BF16), (note_shape, BF16), (note_shape, BF16)],
            got,
            memory,
            packet,
            decay,
            forget_gate_bias,
            alive,
            kept_gain,
        )
        mines.append(own_note)
        notes.append(note)
        got = exchange(sent, ALONG_X)
        if n + 1 < layers:
            sent = kernel(
                functools.partial(output_same_frames_body, layers * columns),
                ((2 * tall, frames, features), BF16),
                got,
                mine,
                theirs,
            )
            shape = (frames * 2 * tall // quad, features)
            got = exchange(sent.reshape(quad, *shape), QUAD)
            got = lax.all_gather(kernel(quad_sum_body, (shape, BF16), got), "far")
            sent = kernel(next_stream_body, ((quad, *shape), BF16), got, x, x_next)
            x = exchange(sent, QUAD).reshape(tall, 2, frames, features)
        else:
            theirs_got = other(jnp.concatenate([got, here[0].reshape(2, BLOCK_LEN, features)], 0), "k")
            sent = kernel(
                functools.partial(output_same_features_body, lax.axis_size("far")),
                ((2 * tall, frames, features), BF16),
                got,
                theirs_got[: 2 * wide],
                output_projection[n],
            )
            shape = (frames * 2 * tall // quad, features)
            got = exchange(sent.reshape(quad, *shape), QUAD)
            sent = kernel(quad_sum_body, (shape, BF16), got).reshape(-1, frames, features)
            notes, sent = lax.optimization_barrier((notes, sent))
            theirs_note = other(jnp.stack(notes), "b")
            current = kernel(
                last_stream_body,
                (stream.shape, BF16),
                exchange(sent, "far"),
                x,
                theirs_got[2 * wide :].reshape(frames, features),
            )
            fresh = kernel(memory_two_body, (memory.shape, F32), memory, *mines, theirs_note)
    return current, fresh


def solution(mesh):
    grp, tp, dp = (mesh.shape[name] for name in ("grp", "tp", "dp"))
    fine = Mesh(
        mesh.devices.reshape(grp, tp // 4, 2, 2, dp // 2, 2), ("grp", *ALONG_TP, "c", "k")
    )
    tp, dp = ALONG_TP, ("c", "k")
    group_tp, group_dp = ("grp", *tp), ("grp", *dp)
    placed = (
        P(group_tp, dp),
        P(group_dp),
        P(None, dp),
        P(None, dp, tp),
        P(None, dp, tp),
        P(None, dp, tp),
        P(None, dp, tp),
        P(None, dp, tp),
        P(None, tp),
        P(None, group_dp, tp),
        P(),
        P(None, tp, dp),
        P(None, group_dp, tp, None),
    )

    return jax.shard_map(
        local,
        mesh=fine,
        in_specs=placed,
        out_specs=(P(group_tp, dp), P(None, group_dp, tp, None)),
        check_vma=False,
    )
```
